512 devices in a mesh: sp: 64 (over z, y), tp: 8 (over x, core).
Axes of the slice: x: 4, y: 8, z: 8, core: 2. Of those that a mesh axis runs over, the one named last changes fastest.
Arguments:
- residual: bfloat16 [8192, 2048], P('sp', 'tp'), may hold values from -24 to 24
- queries: bfloat16 [8192, 2048], P('sp', 'tp'), may hold values from -16 to 16
- key_proj: bfloat16 [8192, 512], P(('sp', 'tp')), may hold values from -8 to 8
- value_proj: bfloat16 [8192, 512], P(('sp', 'tp')), may hold values from -6 to 6
- diff_lambda: float32 [8], replicated, may hold values from 0.3 to 0.8
- head_gain: float32 [256], replicated, may hold values from 0.1 to 1.9
- out_weight: bfloat16 [2048, 2048], P(None, 'tp'), may hold values from -0.125 to 0.125
- norm_gain: float32 [2048], P('tp'), may hold values from 0.1 to 1.9
- up_weight: bfloat16 [2048, 8192], P('sp', 'tp'), may hold values from -0.125 to 0.125
- down_weight: bfloat16 [8192, 2048], P('tp', 'sp'), may hold values from -0.0625 to 0.0625
Outputs:
- layer_out: bfloat16 [8192, 2048], P('sp', 'tp')
The draws below stay inside these ranges and needn't reach their ends.
All inputs are finite; a program needn't handle non-finite values.
Results may differ from the reference program's by a relative error of at most 0.012.
Values may be sent and summed in bfloat16 or wider, within the bound.
A program may use at most 64 MiB of HBM per device.

```python
import jax
import jax.numpy as jnp
from jax import lax

D = 2048
HEADS = 8
KV_HEADS = 2
HEAD_DIM = 128
VALUE_DIM = 256
FF = 8192
TOK_DEV = 128
SEQ = 8192


def draw_residual(key, part):
    base = jax.random.fold_in(key, 11)
    first, second, third = jax.random.split(base, 3)
    noise = jax.random.truncated_normal(first, -3.0, 3.0, (SEQ, D), jnp.float32)
    column = jnp.arange(D, dtype=jnp.float32) / D
    rough = jnp.exp(jax.random.uniform(second, (1, D), jnp.float32, jnp.log(0.8), jnp.log(1.25)))
    col_scale = jnp.exp(jnp.log(0.3) + jnp.log(10.0) * column)[None, :] * rough
    row_scale = jnp.exp(jax.random.uniform(third, (SEQ, 1), jnp.float32, jnp.log(0.5), jnp.log(1.6)))
    return (noise * col_scale * row_scale).astype(jnp.bfloat16)


def drawn_pair(key):
    base = jax.random.fold_in(key, 23)
    streams = jax.random.split(base, 2)
    query_vals = 1.3 * jax.random.truncated_normal(streams[0], -6.0, 6.0, (SEQ, HEADS * 2 * HEAD_DIM), jnp.float32)
    key_vals = 1.3 * jax.random.truncated_normal(streams[1], -6.0, 6.0, (SEQ, KV_HEADS * 2 * HEAD_DIM), jnp.float32)
    return (query_vals, key_vals)


def draw_queries(key, part):
    return drawn_pair(key)[0].astype(jnp.bfloat16)


def draw_key_proj(key, part):
    return drawn_pair(key)[1].astype(jnp.bfloat16)


def levels(own_key, extent, cuts, least, largest):
    def one(position, shards_of):
        heights = jax.random.uniform(jax.random.fold_in(jax.random.fold_in(own_key, 6), position), (shards_of,), jnp.float32, least / len(cuts), largest / len(cuts))
        return jnp.repeat(jnp.exp(heights), extent[position] // shards_of).reshape((-1,) + (1,) * (len(extent) - position - 1))

    loudness = one(*cuts[0])
    for cut in cuts[1:]:
        loudness = loudness * one(*cut)
    return loudness


def normal_values(own_key, shape, deviation, most, shards=(), held_as=jnp.bfloat16):
    values = jax.random.normal(own_key, shape, jnp.float32) * deviation
    if len(shards) > 0:
        values = levels(own_key, shape, shards, -0.22, 0.18) * values
    return jnp.clip(values, min=-most, max=most).astype(held_as)


def setup_inputs(seed: int = 0) -> dict:
    key_list = jax.random.split(jax.random.key(seed), 11)
    residual = draw_residual(jax.random.fold_in(key_list[10], 71), 0)
    queries = draw_queries(jax.random.fold_in(key_list[10], 71), 0)
    key_proj = draw_key_proj(jax.random.fold_in(key_list[10], 71), 0)
    value_proj = normal_values(key_list[3], (SEQ, KV_HEADS * VALUE_DIM), 1.0, 6.0, ((0, 512),))
    diff_lambda = jnp.clip(jax.random.uniform(key_list[4], (HEADS,), jnp.float32, 0.3, 0.8), 0.3, 0.8)
    head_gain = jnp.clip(1.0 + 0.18 * jax.random.normal(key_list[5], (VALUE_DIM,), jnp.float32), 0.1, 1.9)
    out_weight = normal_values(key_list[6], (HEADS * VALUE_DIM, D), (HEADS * VALUE_DIM) ** -0.5, 0.125, ((1, 8),))
    norm_gain = jnp.clip(1.0 + 0.18 * jax.random.normal(key_list[7], (D,), jnp.float32), 0.1, 1.9)
    up_weight = normal_values(key_list[8], (D, FF), D ** -0.5, 0.125, ((0, 64), (1, 8)))
    down_weight = normal_values(key_list[9], (FF, D), FF ** -0.5, 0.0625, ((0, 8), (1, 64)))
    return dict(residual=residual, queries=queries, key_proj=key_proj, value_proj=value_proj, diff_lambda=diff_lambda, head_gain=head_gain, out_weight=out_weight, norm_gain=norm_gain, up_weight=up_weight, down_weight=down_weight)


epsilon = 1e-06

def reference(residual, queries, key_proj, value_proj, diff_lambda, head_gain, out_weight, norm_gain, up_weight, down_weight):
    per_group = HEADS // KV_HEADS
    seq_len = queries.shape[0]
    scaling = HEAD_DIM ** (-0.5)
    key_grid = key_proj.astype(jnp.float32).reshape(seq_len, KV_HEADS, 2, HEAD_DIM)
    value_grid = value_proj.astype(jnp.float32).reshape(seq_len, KV_HEADS, VALUE_DIM)
    lambdas = diff_lambda.reshape(KV_HEADS, per_group, 1, 1)
    blocks = queries.reshape(seq_len // TOK_DEV, TOK_DEV, KV_HEADS, per_group, 2, HEAD_DIM)

    def one_block(query_block):
        query_float = query_block.astype(jnp.float32)
        scores = jnp.einsum('qagcd,kacd->agcqk', query_float, key_grid) * scaling
        highest = lax.optimization_barrier(jnp.max(scores, axis=-1, keepdims=True))
        weights = jnp.exp(scores - highest)
        totals = lax.optimization_barrier(jnp.sum(weights, axis=-1))
        rounded = lax.optimization_barrier(weights.astype(jnp.bfloat16)).astype(jnp.float32)
        summed = jnp.einsum('agcqk,kae->agcqe', rounded, value_grid)
        per_map = summed / totals[..., None]
        difference = per_map[:, :, 0] - lambdas * per_map[:, :, 1]
        normed = difference * lax.rsqrt(lax.optimization_barrier(jnp.mean(difference * difference, axis=-1, keepdims=True)) + epsilon) * head_gain
        return normed.astype(jnp.bfloat16).reshape(HEADS, TOK_DEV, VALUE_DIM)
    outputs = lax.map(one_block, blocks)
    head_outputs = outputs.transpose(1, 0, 2, 3).reshape(HEADS, seq_len, VALUE_DIM)
    out_grid = out_weight.reshape(HEADS, VALUE_DIM, D)
    projected = jnp.einsum('hse,hed->sd', head_outputs.astype(jnp.float32), out_grid.astype(jnp.float32))
    after_mix = residual.astype(jnp.float32) + projected
    normed = (after_mix * lax.rsqrt(lax.optimization_barrier(jnp.mean(after_mix * after_mix, axis=1, keepdims=True)) + epsilon) * norm_gain).astype(jnp.bfloat16)
    hidden = jnp.dot(normed, up_weight, preferred_element_type=jnp.float32)
    activated = jnp.square(jax.nn.relu(hidden)).astype(jnp.bfloat16)
    mixed = jnp.dot(activated, down_weight, preferred_element_type=jnp.float32)
    return (after_mix + mixed).astype(jnp.bfloat16)
```

```python
import jax
import jax.numpy as jnp
from jax import lax
from jax.experimental import pallas as pl
from jax.experimental.pallas import tpu as pltpu
from jax.sharding import PartitionSpec as P

D = 2048
HEADS = 8
HEAD_DIM = 128
VALUE_DIM = 256
RING = 8
TP = 8
ROWS = 128
EPSILON = 1e-06
MESH = pl.DeviceIdType.MESH
F32 = jnp.float32
BF16 = jnp.bfloat16
LOG_SCALE = HEAD_DIM ** (-0.5) * 1.4426950408889634
NT = (((1,), (1,)), ((), ()))


def wrap(i):
    return lax.rem(i + RING, RING)


class Gather:
    def __init__(self, first, second, y, z, tp, send, near, far):
        self.arrays = (first, second)
        self.y, self.z, self.tp = y, z, tp
        self.send, self.near, self.far = send, near, far

    def chunk(self, kind, p2, p1):
        array = self.arrays[kind]
        return array.at[p2 * RING + p1] if kind == 0 else array.at[p1 * RING + p2]

    def me1(self, kind):
        return self.y if kind == 0 else self.z

    def me2(self, kind):
        return self.z if kind == 0 else self.y

    def device(self, along_y, step):
        if along_y:
            return (self.z * RING + wrap(self.y + step), self.tp)
        return (wrap(self.z + step) * RING + self.y, self.tp)

    def near_copy(self, kind, way, s, at):
        c = self.chunk(kind, self.me2(kind), at)
        return pltpu.make_async_remote_copy(
            src_ref=c, dst_ref=c, send_sem=self.send.at[kind],
            recv_sem=self.near.at[kind, way, s],
            device_id=self.device(kind == 0, 1 - 2 * way), device_id_type=MESH)

    def far_copy(self, kind, way, s, at2, at1):
        c = self.chunk(kind, at2, at1)
        return pltpu.make_async_remote_copy(
            src_ref=c, dst_ref=c, send_sem=self.send.at[kind],
            recv_sem=self.far.at[kind, way, s, at1],
            device_id=self.device(kind == 1, 1 - 2 * way), device_id_type=MESH)

    def open_chunk(self, kind, at1):
        for way in range(2):
            self.far_copy(kind, way, 0, self.me2(kind), at1).start()

    def begin(self):
        for kind in range(2):
            for way in range(2):
                self.near_copy(kind, way, 0, self.me1(kind)).start()
        for kind in range(2):
            self.open_chunk(kind, self.me1(kind))

    def near_step(self, u):
        for way in range(2):
            if way == 1 and u == 4:
                continue
            for kind in range(2):
                at = wrap(self.me1(kind) - u * (1 - 2 * way))
                self.near_copy(kind, way, u - 1, at).wait_recv()
                if u < 4 - way:
                    self.near_copy(kind, way, u, at).start()
                self.open_chunk(kind, at)

    def far_step(self, s, j):
        half = lax.div(j + 1, 2)
        offset = half * (1 - 2 * lax.rem(j, 2))
        for way in range(2):
            mine = (j < 4) if way == 0 else (j >= 4)
            for kind in range(2):
                at1 = wrap(self.me1(kind) + offset)
                at2 = wrap(self.me2(kind) - s * (1 - 2 * way))

                def arrive():
                    self.far_copy(kind, way, s - 1, at2, at1).wait_recv()

                def forward():
                    self.far_copy(kind, way, s, at2, at1).start()

                if s < 4:
                    arrive()
                else:
                    pl.when(mine)(arrive)
                if s < 3:
                    forward()
                elif s == 3:
                    pl.when(mine)(forward)

    def far_steps(self, s, low, high):
        @pl.loop(low, high)
        def _(j):
            self.far_step(s, j)

    def finish(self):
        for kind in range(2):
            part = self.arrays[kind].at[0 : RING * RING - 1]
            pltpu.make_async_remote_copy(
                src_ref=part, dst_ref=part, send_sem=self.send.at[kind],
                recv_sem=self.near.at[kind, 0, 0],
                device_id=self.device(True, 1), device_id_type=MESH).wait_send()


def kernel(
    res_ref, q_ref, key_ref, val_ref, lam_ref, hgain_ref, ow_ref, ngain_ref, up_ref, down_ref,
    out_ref,
    k_all, v_all, up_all, dn_all, q_all, st_all, d_out, d_all, ho_all, an_all, sq_all,
    rs_out, rs_all, o_scr, am_scr, hid_scr,
    kv_send, kv_near, kv_far, w_send, w_near, w_far, x_send, x_recv,
):
    sp, tp = lax.axis_index("sp"), lax.axis_index("tp")
    z, y = lax.div(sp, RING), lax.rem(sp, RING)
    kv = Gather(k_all, v_all, y, z, tp, kv_send, kv_near, kv_far)
    w = Gather(up_all, dn_all, y, z, tp, w_send, w_near, w_far)

    barrier = pltpu.get_barrier_semaphore()

    @pl.loop(1, TP)
    def _(p):
        pl.semaphore_signal(barrier, inc=1, device_id=(sp, wrap(tp + p)), device_id_type=MESH)

    for along_y in (True, False):
        for step in (1, -1):
            pl.semaphore_signal(barrier, inc=1, device_id=kv.device(along_y, step), device_id_type=MESH)

    k_all[sp] = key_ref[...]
    v_all[sp] = val_ref[...]
    up_all[sp] = up_ref[...]
    rows = lax.broadcasted_iota(jnp.int32, (32, 32), 0)
    cols = lax.broadcasted_iota(jnp.int32, (32, 32), 1)
    eye = jnp.where(rows == cols, 1.0, 0.0).astype(BF16)
    dn_all[sp] = lax.dot_general(eye, down_ref[...], NT, preferred_element_type=F32).astype(BF16)
    q_all[tp] = q_ref[...]

    pl.semaphore_wait(barrier, TP - 1 + 4)

    def x_copy(k, src, dst, slot, peer):
        return pltpu.make_async_remote_copy(
            src_ref=src, dst_ref=dst.at[slot], send_sem=x_send.at[k], recv_sem=x_recv.at[k, slot],
            device_id=(sp, peer), device_id_type=MESH)

    def x_share(k, array):
        @pl.loop(1, TP)
        def _(p):
            x_copy(k, array.at[tp], array, tp, wrap(tp + p)).start()

    def x_wait(k, array):
        @pl.loop(1, TP)
        def _(p):
            slot = wrap(tp - p)
            x_copy(k, array.at[slot], array, slot, slot).wait_recv()

    def x_sent(k, array):
        part = array.at[0:7]
        pltpu.make_async_remote_copy(
            src_ref=part, dst_ref=part, send_sem=x_send.at[k], recv_sem=x_recv.at[k, 0],
            device_id=(sp, wrap(tp + 1)), device_id_type=MESH).wait_send()

    kv.begin()
    x_share(0, q_all)
    w.begin()
    for u in range(1, 5):
        kv.near_step(u)
    for s in range(1, 4):
        kv.far_steps(s, 0, 8)
        w.near_step(s)
    w.near_step(4)
    kv.far_steps(4, 0, 8)
    x_wait(0, q_all)

    lane = lax.broadcasted_iota(jnp.int32, (ROWS, 128), 1)

    def attend(gc, stats):
        g, c = lax.div(gc, 2), lax.rem(gc, 2)
        q = q_all[pl.ds(4 * g, 4), :, pl.ds(pl.multiple_of(c * 128, 128), 128)].reshape(4 * ROWS, 128)
        k = k_all[:, :, pl.ds(pl.multiple_of(gc * 128, 128), 128)].reshape(1024, 128)
        v = v_all[:, :, pl.ds(pl.multiple_of(g * 256, 256), 256)].reshape(1024, 256)
        s = lax.dot_general(q, k, NT, preferred_element_type=F32)
        m = jnp.max(s, axis=1, keepdims=True)
        p = jnp.exp2((s - m) * LOG_SCALE)
        t = jnp.sum(p, axis=1, keepdims=True)
        o = jnp.dot(p.astype(BF16), v, preferred_element_type=F32)
        m = m * LOG_SCALE
        for i in range(4):
            at = (4 * g + i) * 2 + c
            o_scr[at] = o[i * ROWS : (i + 1) * ROWS]
            stats = jnp.where(lane == at, m[i * ROWS : (i + 1) * ROWS], stats)
            stats = jnp.where(lane == at + 16, t[i * ROWS : (i + 1) * ROWS], stats)
        w.far_step(1, 2 * gc)
        w.far_step(1, 2 * gc + 1)
        return stats

    stats = lax.fori_loop(0, 4, attend, jnp.zeros((ROWS, 128), F32))
    st_all[tp] = jnp.transpose(stats)[0:32]
    w.far_steps(2, 0, 1)
    x_share(1, st_all)
    w.far_steps(2, 1, 3)
    x_wait(1, st_all)

    every = st_all[...]
    maxima, totals = every[:, 0:16], every[:, 16:32]
    highest = jnp.max(maxima, axis=0)
    total = jnp.sum(jnp.exp2(maxima - highest[None]) * totals, axis=0)
    mine = st_all[tp]
    coef = jnp.exp2(mine[0:16] - highest) / total
    row = lax.broadcasted_iota(jnp.int32, (16, 128), 0)
    factor = jnp.ones((16, 128), F32)
    for h in range(HEADS):
        factor = jnp.where(row == 2 * h + 1, -lam_ref[h], factor)
    coef = jnp.concatenate([coef * factor, jnp.zeros((112, 128), F32)], axis=0)
    coef = jnp.transpose(coef)
    for h in range(HEADS):
        part = o_scr[2 * h] * coef[:, 2 * h : 2 * h + 1] + o_scr[2 * h + 1] * coef[:, 2 * h + 1 : 2 * h + 2]
        d_out[h] = part.astype(BF16)
    d_all[tp] = d_out[tp]

    @pl.loop(1, TP)
    def _(p):
        peer = wrap(tp + p)
        x_copy(2, d_out.at[peer], d_all, tp, peer).start()

    w.far_steps(2, 3, 8)
    x_wait(2, d_all)
    difference = jnp.sum(d_all[...].astype(F32), axis=0)
    square = jnp.mean(difference * difference, axis=-1, keepdims=True)
    ho_all[tp] = (difference * lax.rsqrt(square + EPSILON) * hgain_ref[...]).astype(BF16)
    w.far_steps(3, 0, 1)
    x_share(3, ho_all)
    w.far_steps(3, 1, 4)
    x_wait(3, ho_all)
    projected = jnp.zeros((ROWS, 256), F32)
    for h in range(HEADS):
        projected += jnp.dot(ho_all[h], ow_ref[h * 256 : (h + 1) * 256], preferred_element_type=F32)
    after_mix = res_ref[...].astype(F32) + projected
    am_scr[...] = after_mix
    an_all[tp] = (after_mix * ngain_ref[...]).astype(BF16)
    squares = jnp.sum(after_mix * after_mix, axis=1, keepdims=True)
    sq_all[tp] = jnp.transpose(jnp.broadcast_to(squares, (ROWS, 128)))[0:8]
    w.far_steps(3, 4, 5)
    x_share(4, an_all)
    x_share(5, sq_all)
    w.far_steps(3, 5, 8)
    x_wait(4, an_all)
    x_wait(5, sq_all)
    squares = jnp.sum(sq_all[...], axis=0)
    squares = jnp.transpose(jnp.broadcast_to(squares[0:1], (128, 128)))[:, 0:1]
    scale = lax.rsqrt(squares / D + EPSILON)
    w.far_steps(4, 0, 8)

    hid_scr[...] = jnp.zeros_like(hid_scr)

    @pl.loop(0, TP)
    def _(t):
        hid_scr[...] += jnp.dot(an_all[t], up_all[pl.ds(t * RING, RING)].reshape(256, 1024), preferred_element_type=F32)

    activated = jnp.square(jax.nn.relu(hid_scr[...] * scale)).astype(BF16)

    def mixed(t):
        return lax.dot_general(activated, dn_all[pl.ds(t * RING, RING)].reshape(256, 1024), NT, preferred_element_type=F32)

    def rs_copy(p):
        peer = wrap(tp + p)
        return x_copy(6, rs_out.at[peer], rs_all, tp, peer)

    for p in range(1, TP):
        peer = wrap(tp + p)
        rs_out[peer] = mixed(peer).astype(BF16)
        if p > 1:
            rs_copy(p - 1).start()
    own = am_scr[...] + mixed(tp)
    rs_copy(TP - 1).start()
    rs_all[tp] = jnp.zeros((ROWS, 256), BF16)
    x_wait(6, rs_all)
    out_ref[...] = (own + jnp.sum(rs_all[...].astype(F32), axis=0)).astype(BF16)

    kv.finish()
    w.finish()
    for k, array in enumerate((q_all, st_all, d_out, ho_all, an_all, sq_all, rs_out)):
        x_sent(k, array)


def on_device(residual, queries, key_proj, value_proj, diff_lambda, head_gain, out_weight, norm_gain, up_weight, down_weight):
    vmem = pl.BlockSpec(memory_space=pltpu.VMEM)
    smem = pl.BlockSpec(memory_space=pltpu.SMEM)
    block = (TP, ROWS, 256)
    dma = pltpu.SemaphoreType.DMA
    return pl.pallas_call(
        kernel,
        out_shape=jax.ShapeDtypeStruct((ROWS, 256), BF16),
        in_specs=[vmem, vmem, vmem, vmem, smem] + [vmem] * 5,
        out_specs=vmem,
        scratch_shapes=[
            pltpu.VMEM((RING * RING, 16, 512), BF16),
            pltpu.VMEM((RING * RING, 16, 512), BF16),
            pltpu.VMEM((RING * RING, 32, 1024), BF16),
            pltpu.VMEM((RING * RING, 32, 1024), BF16),
            pltpu.VMEM(block, BF16),
            pltpu.VMEM((TP, 32, 128), F32),
            pltpu.VMEM(block, BF16),
            pltpu.VMEM(block, BF16),
            pltpu.VMEM(block, BF16),
            pltpu.VMEM(block, BF16),
            pltpu.VMEM((TP, 8, 128), F32),
            pltpu.VMEM(block, BF16),
            pltpu.VMEM(block, BF16),
            pltpu.VMEM((16, ROWS, 256), F32),
            pltpu.VMEM((ROWS, 256), F32),
            pltpu.VMEM((ROWS, 1024), F32),
            dma((2,)), dma((2, 2, 4)), dma((2, 2, 4, 8)),
            dma((2,)), dma((2, 2, 4)), dma((2, 2, 4, 8)),
            dma((7,)), dma((7, TP)),
        ],
        compiler_params=pltpu.CompilerParams(
            collective_id=0, has_side_effects=True, vmem_limit_bytes=48 * 1024 * 1024),
    )(residual, queries, key_proj, value_proj, diff_lambda, head_gain.reshape(1, 256), out_weight,
      norm_gain.reshape(1, 256), up_weight, down_weight)


def solution(mesh):
    return jax.shard_map(
        on_device,
        mesh=mesh,
        in_specs=(
            P("sp", "tp"),
            P("sp", "tp"),
            P(("sp", "tp"), None),
            P(("sp", "tp"), None),
            P(),
            P(),
            P(None, "tp"),
            P("tp"),
            P("sp", "tp"),
            P("tp", "sp"),
        ),
        out_specs=P("sp", "tp"),
        check_vma=False,
    )
```

```python
import jax
import jax.numpy as jnp
from jax import lax
from jax.experimental import pallas as pl
from jax.experimental.pallas import tpu as pltpu
from jax.sharding import PartitionSpec as P

D = 2048
HEADS = 8
HEAD_DIM = 128
VALUE_DIM = 256
RING = 8
TP = 8
ROWS = 128
EPSILON = 1e-06
MESH = pl.DeviceIdType.MESH
F32 = jnp.float32
BF16 = jnp.bfloat16
LOG_SCALE = HEAD_DIM ** (-0.5) * 1.4426950408889634
NT = (((1,), (1,)), ((), ()))


def wrap(i):
    return lax.rem(i + RING, RING)


class Gather:
    def __init__(self, first, second, y, z, tp, send, near, far, direct):
        self.direct = direct
        self.arrays = (first, second)
        self.y, self.z, self.tp = y, z, tp
        self.send, self.near, self.far = send, near, far

    def chunk(self, kind, p2, p1):
        array = self.arrays[kind]
        return array.at[p2 * RING + p1] if kind == 0 else array.at[p1 * RING + p2]

    def me1(self, kind):
        return self.y if kind == 0 else self.z

    def me2(self, kind):
        return self.z if kind == 0 else self.y

    def device(self, along_y, step):
        if along_y:
            return (self.z * RING + wrap(self.y + step), self.tp)
        return (wrap(self.z + step) * RING + self.y, self.tp)

    def near_copy(self, kind, way, s, at):
        c = self.chunk(kind, self.me2(kind), at)
        return pltpu.make_async_remote_copy(
            src_ref=c, dst_ref=c, send_sem=self.send.at[kind],
            recv_sem=self.near.at[kind, way, s],
            device_id=self.device(kind == 0, (1 - 2 * way) * (s + 1 if self.direct else 1)),
            device_id_type=MESH)

    def far_copy(self, kind, way, s, at2, at1):
        c = self.chunk(kind, at2, at1)
        return pltpu.make_async_remote_copy(
            src_ref=c, dst_ref=c, send_sem=self.send.at[kind],
            recv_sem=self.far.at[kind, way, s, at1],
            device_id=self.device(kind == 1, 1 - 2 * way), device_id_type=MESH)

    def open_chunk(self, kind, at1):
        for way in range(2):
            self.far_copy(kind, way, 0, self.me2(kind), at1).start()

    def begin(self):
        for s in range(4 if self.direct else 1):
            for kind in range(2):
                for way in range(2 if s < 3 else 1):
                    self.near_copy(kind, way, s, self.me1(kind)).start()
        for kind in range(2):
            self.open_chunk(kind, self.me1(kind))

    def near_step(self, u):
        for way in range(2):
            if way == 1 and u == 4:
                continue
            for kind in range(2):
                at = wrap(self.me1(kind) - u * (1 - 2 * way))
                self.near_copy(kind, way, u - 1, at).wait_recv()
                if u < 4 - way and not self.direct:
                    self.near_copy(kind, way, u, at).start()
                self.open_chunk(kind, at)

    def far_step(self, s, j):
        half = lax.div(j + 1, 2)
        offset = half * (1 - 2 * lax.rem(j, 2))
        for way in range(2):
            mine = lax.rem(j, 2) == way
            for kind in range(2):
                at1 = wrap(self.me1(kind) + offset)
                at2 = wrap(self.me2(kind) - s * (1 - 2 * way))

                def arrive():
                    self.far_copy(kind, way, s - 1, at2, at1).wait_recv()

                def forward():
                    self.far_copy(kind, way, s, at2, at1).start()

                if s < 4:
                    arrive()
                else:
                    pl.when(mine)(arrive)
                if s < 3:
                    forward()
                elif s == 3:
                    pl.when(mine)(forward)

    def far_steps(self, s, low, high):
        @pl.loop(low, high)
        def _(j):
            self.far_step(s, j)

    def finish(self):
        for kind in range(2):
            part = self.arrays[kind].at[0 : RING * RING - 1]
            pltpu.make_async_remote_copy(
                src_ref=part, dst_ref=part, send_sem=self.send.at[kind],
                recv_sem=self.near.at[kind, 0, 0],
                device_id=self.device(True, 1), device_id_type=MESH).wait_send()


def kernel(
    res_ref, q_ref, key_ref, val_ref, lam_ref, hgain_ref, ow_ref, ngain_ref, up_ref, down_ref,
    out_ref,
    k_all, v_all, up_all, dn_all, q_all, st_all, ho_all, an_all, sq_all,
    pre_out, pre_in, rs_out, rs_all, keep, o_scr, am_scr, hid_scr,
    kv_send, kv_near, kv_far, w_send, w_near, w_far, x_send, x_recv, pre_send, pre_recv,
):
    sp, tp = lax.axis_index("sp"), lax.axis_index("tp")
    z, y = lax.div(sp, RING), lax.rem(sp, RING)
    kv = Gather(k_all, v_all, y, z, tp, kv_send, kv_near, kv_far, True)
    w = Gather(up_all, dn_all, y, z, tp, w_send, w_near, w_far, False)

    barrier = pltpu.get_barrier_semaphore()

    @pl.loop(1, TP)
    def _(p):
        pl.semaphore_signal(barrier, inc=1, device_id=(sp, wrap(tp + p)), device_id_type=MESH)

    @pl.loop(1, RING)
    def _(p):
        for along_y in (True, False):
            pl.semaphore_signal(barrier, inc=1, device_id=kv.device(along_y, p), device_id_type=MESH)

    k_all[sp] = key_ref[...]
    v_all[sp] = val_ref[...]
    up_all[sp] = up_ref[...]
    rows = lax.broadcasted_iota(jnp.int32, (32, 32), 0)
    cols = lax.broadcasted_iota(jnp.int32, (32, 32), 1)
    eye = jnp.where(rows == cols, 1.0, 0.0).astype(BF16)
    dn_all[sp] = lax.dot_general(eye, down_ref[...], NT, preferred_element_type=F32).astype(BF16)
    q_all[tp] = q_ref[...]

    pl.semaphore_wait(barrier, TP - 1 + 2 * (RING - 1))

    x, c = lax.div(tp, 2), lax.rem(tp, 2)

    def chip(step):
        return lax.rem(x + step + 4, 4)

    def tp_of(step):
        return chip(step) * 2 + c

    partner = x * 2 + 1 - c

    def x_copy(k, src, dst, slot, peer):
        return pltpu.make_async_remote_copy(
            src_ref=src, dst_ref=dst.at[slot], send_sem=x_send.at[k], recv_sem=x_recv.at[k, slot],
            device_id=(sp, peer), device_id_type=MESH)

    def x_arrived(k, dst, slot):
        x_copy(k, dst.at[slot], dst, slot, partner).wait_recv()

    def share(k, array):
        for step in (2, 1, 3):
            x_copy(k, array.at[tp], array, tp, tp_of(step)).start()
        x_copy(k, array.at[tp], array, tp, partner).start()

    def relay(k, array):
        for step in (1, 3, 2):
            slot = tp_of(step)
            x_arrived(k, array, slot)
            x_copy(k, array.at[slot], array, slot, partner).start()

    def collect(k, array):
        for step in (0, 1, 3, 2):
            x_arrived(k, array, chip(step) * 2 + 1 - c)

    def x_sent(k, part):
        pltpu.make_async_remote_copy(
            src_ref=part, dst_ref=part, send_sem=x_send.at[k], recv_sem=x_recv.at[k, 0],
            device_id=(sp, partner), device_id_type=MESH).wait_send()

    events = [(s, j) for s in range(1, 5) for j in range(8)]

    def pump(count):
        for _ in range(count):
            s, j = events.pop(0)
            w.far_step(s, j)

    def reduce_pair(k, produce, gone):
        for i in range(4):
            pre_out[k, i] = produce(i, 2 * i + 1 - c).astype(BF16)
        copy = pltpu.make_async_remote_copy(
            src_ref=pre_out.at[k], dst_ref=pre_in.at[k], send_sem=pre_send.at[k], recv_sem=pre_recv.at[k],
            device_id=(sp, partner), device_id_type=MESH)
        copy.start()
        for i in range(4):
            keep[i] = produce(i, 2 * i + c)
        copy.wait_recv()
        for step in (2, 1, 3):
            i = chip(step)
            rs_out[k, i] = (keep[i] + pre_in[k, i].astype(F32)).astype(BF16)
        for step in (2, 1, 3):
            i = chip(step)
            x_copy(gone, rs_out.at[k, i], rs_all.at[k], x, tp_of(step)).start()
        return keep[x] + pre_in[k, x].astype(F32)

    def reduce_rest(k, gone, total):
        for step in (1, 3, 2):
            i = chip(step)
            x_arrived(gone, rs_all.at[k], i)
            total += rs_all[k, i].astype(F32)
        return total

    kv.begin()
    share(0, q_all)
    w.begin()
    for u in range(1, 5):
        kv.near_step(u)
    relay(0, q_all)
    for s in range(1, 4):
        kv.far_steps(s, 0, 8)
        w.near_step(s)
    w.near_step(4)
    kv.far_steps(4, 0, 8)
    collect(0, q_all)

    lane = lax.broadcasted_iota(jnp.int32, (ROWS, 128), 1)
    stats = jnp.zeros((ROWS, 128), F32)
    for gc in range(4):
        g, m_c = gc // 2, gc % 2
        q = q_all[4 * g : 4 * g + 4, :, m_c * 128 : m_c * 128 + 128].reshape(4 * ROWS, 128)
        k = k_all[:, :, gc * 128 : gc * 128 + 128].reshape(1024, 128)
        v = v_all[:, :, g * 256 : g * 256 + 256].reshape(1024, 256)
        s = lax.dot_general(q, k, NT, preferred_element_type=F32)
        m = jnp.max(s, axis=1, keepdims=True)
        p = jnp.exp2((s - m) * LOG_SCALE)
        t = jnp.sum(p, axis=1, keepdims=True)
        o = jnp.dot(p.astype(BF16), v, preferred_element_type=F32)
        m = m * LOG_SCALE
        for i in range(4):
            at = (4 * g + i) * 2 + m_c
            o_scr[at] = o[i * ROWS : (i + 1) * ROWS]
            stats = jnp.where(lane == at, m[i * ROWS : (i + 1) * ROWS], stats)
            stats = jnp.where(lane == at + 16, t[i * ROWS : (i + 1) * ROWS], stats)
        pump(2)

    st_all[tp] = jnp.transpose(stats)[0:32]
    pump(1)
    for step in (2, 1, 3):
        for core in range(2):
            x_copy(1, st_all.at[tp], st_all, tp, chip(step) * 2 + core).start()
    x_copy(1, st_all.at[tp], st_all, tp, partner).start()
    pump(2)
    x_arrived(1, st_all, partner)
    for step in (1, 3, 2):
        for core in range(2):
            x_arrived(1, st_all, chip(step) * 2 + core)

    every = st_all[...]
    maxima, totals = every[:, 0:16], every[:, 16:32]
    highest = jnp.max(maxima, axis=0)
    total = jnp.sum(jnp.exp2(maxima - highest[None]) * totals, axis=0)
    mine = st_all[tp]
    coef = jnp.exp2(mine[0:16] - highest) / total
    row = lax.broadcasted_iota(jnp.int32, (16, 128), 0)
    factor = jnp.ones((16, 128), F32)
    for h in range(HEADS):
        factor = jnp.where(row == 2 * h + 1, -lam_ref[h], factor)
    coef = jnp.concatenate([coef * factor, jnp.zeros((112, 128), F32)], axis=0)
    coef = jnp.transpose(coef)

    def differ(i, h):
        even = lax.rem(h, 2) == 0
        first = jnp.where(even, coef[:, 4 * i : 4 * i + 1], coef[:, 4 * i + 2 : 4 * i + 3])
        second = jnp.where(even, coef[:, 4 * i + 1 : 4 * i + 2], coef[:, 4 * i + 3 : 4 * i + 4])
        return o_scr[2 * h] * first + o_scr[2 * h + 1] * second

    difference = reduce_pair(0, differ, 2)
    pump(4)
    difference = reduce_rest(0, 2, difference)
    square = jnp.mean(difference * difference, axis=-1, keepdims=True)
    ho_all[tp] = (difference * lax.rsqrt(square + EPSILON) * hgain_ref[...]).astype(BF16)
    pump(1)
    share(3, ho_all)
    pump(3)
    relay(3, ho_all)
    pump(2)
    collect(3, ho_all)
    projected = jnp.zeros((ROWS, 256), F32)
    for h in range(HEADS):
        projected += jnp.dot(ho_all[h], ow_ref[h * 256 : (h + 1) * 256], preferred_element_type=F32)
    after_mix = res_ref[...].astype(F32) + projected
    am_scr[...] = after_mix
    an_all[tp] = (after_mix * ngain_ref[...]).astype(BF16)
    squares = jnp.sum(after_mix * after_mix, axis=1, keepdims=True)
    sq_all[tp] = jnp.transpose(jnp.broadcast_to(squares, (ROWS, 128)))[0:8]
    pump(1)
    share(4, an_all)
    share(5, sq_all)
    pump(2)
    relay(4, an_all)
    relay(5, sq_all)
    pump(2)
    collect(4, an_all)
    collect(5, sq_all)
    squares = jnp.sum(sq_all[...], axis=0)
    squares = jnp.transpose(jnp.broadcast_to(squares[0:1], (128, 128)))[:, 0:1]
    scale = lax.rsqrt(squares / D + EPSILON)
    pump(len(events))

    hid_scr[...] = jnp.zeros_like(hid_scr)

    @pl.loop(0, TP)
    def _(t):
        hid_scr[...] += jnp.dot(
            an_all[t], up_all[pl.ds(t * RING, RING)].reshape(256, 1024), preferred_element_type=F32)

    activated = jnp.square(jax.nn.relu(hid_scr[...] * scale)).astype(BF16)

    def mixed(i, t):
        weights = dn_all[pl.ds(t * RING, RING)].reshape(256, 1024)
        return lax.dot_general(activated, weights, NT, preferred_element_type=F32)

    own = reduce_pair(1, mixed, 6) + am_scr[...]
    out_ref[...] = reduce_rest(1, 6, own).astype(BF16)

    kv.finish()
    w.finish()
    for k, array in ((0, q_all), (1, st_all), (3, ho_all), (4, an_all), (5, sq_all)):
        x_sent(k, array.at[0:7])
    for k, gone in ((0, 2), (1, 6)):
        x_sent(gone, rs_out.at[k, 0:3])
        pltpu.make_async_remote_copy(
            src_ref=pre_out.at[k], dst_ref=pre_in.at[k], send_sem=pre_send.at[k], recv_sem=pre_recv.at[k],
            device_id=(sp, partner), device_id_type=MESH).wait_send()


def on_device(residual, queries, key_proj, value_proj, diff_lambda, head_gain, out_weight, norm_gain, up_weight, down_weight):
    vmem = pl.BlockSpec(memory_space=pltpu.VMEM)
    smem = pl.BlockSpec(memory_space=pltpu.SMEM)
    block = (TP, ROWS, 256)
    dma = pltpu.SemaphoreType.DMA
    return pl.pallas_call(
        kernel,
        out_shape=jax.ShapeDtypeStruct((ROWS, 256), BF16),
        in_specs=[vmem, vmem, vmem, vmem, smem] + [vmem] * 5,
        out_specs=vmem,
        scratch_shapes=[
            pltpu.VMEM((RING * RING, 16, 512), BF16),
            pltpu.VMEM((RING * RING, 16, 512), BF16),
            pltpu.VMEM((RING * RING, 32, 1024), BF16),
            pltpu.VMEM((RING * RING, 32, 1024), BF16),
            pltpu.VMEM(block, BF16),
            pltpu.VMEM((TP, 32, 128), F32),
            pltpu.VMEM(block, BF16),
            pltpu.VMEM(block, BF16),
            pltpu.VMEM((TP, 8, 128), F32),
            pltpu.VMEM((2, 4, ROWS, 256), BF16),
            pltpu.VMEM((2, 4, ROWS, 256), BF16),
            pltpu.VMEM((2, 4, ROWS, 256), BF16),
            pltpu.VMEM((2, 4, ROWS, 256), BF16),
            pltpu.VMEM((4, ROWS, 256), F32),
            pltpu.VMEM((16, ROWS, 256), F32),
            pltpu.VMEM((ROWS, 256), F32),
            pltpu.VMEM((ROWS, 1024), F32),
            dma((2,)), dma((2, 2, 4)), dma((2, 2, 4, 8)),
            dma((2,)), dma((2, 2, 4)), dma((2, 2, 4, 8)),
            dma((7,)), dma((7, TP)), dma((2,)), dma((2,)),
        ],
        compiler_params=pltpu.CompilerParams(
            collective_id=0, has_side_effects=True, vmem_limit_bytes=48 * 1024 * 1024),
    )(residual, queries, key_proj, value_proj, diff_lambda, head_gain.reshape(1, 256), out_weight,
      norm_gain.reshape(1, 256), up_weight, down_weight)


def solution(mesh):
    return jax.shard_map(
        on_device,
        mesh=mesh,
        in_specs=(
            P("sp", "tp"),
            P("sp", "tp"),
            P(("sp", "tp"), None),
            P(("sp", "tp"), None),
            P(),
            P(),
            P(None, "tp"),
            P("tp"),
            P("sp", "tp"),
            P("tp", "sp"),
        ),
        out_specs=P("sp", "tp"),
        check_vma=False,
    )
```

```python
import jax
import jax.numpy as jnp
from jax import lax
from jax.experimental import pallas as pl
from jax.experimental.pallas import tpu as pltpu
from jax.sharding import PartitionSpec as P

D = 2048
HEADS = 8
HEAD_DIM = 128
RING = 8
TP = 8
ROWS = 128
EPSILON = 1e-06
MESH = pl.DeviceIdType.MESH
F32 = jnp.float32
BF16 = jnp.bfloat16
LOG_SCALE = HEAD_DIM ** (-0.5) * 1.4426950408889634
NT = (((1,), (1,)), ((), ()))


def wrap(i):
    return lax.rem(i + RING, RING)


class Gather:
    def __init__(self, first, second, y, z, tp, sems, direct, group):
        self.arrays = (first, second)
        self.y, self.z, self.tp = y, z, tp
        self.send, self.near, self.far = sems
        self.direct, self.group = direct, group

    def me1(self, kind):
        return self.y if kind == 0 else self.z

    def me2(self, kind):
        return self.z if kind == 0 else self.y

    def device(self, along_y, step):
        if along_y:
            return (self.z * RING + wrap(self.y + step), self.tp)
        return (wrap(self.z + step) * RING + self.y, self.tp)

    def near_copy(self, kind, way, s, at):
        c = self.arrays[kind].at[self.me2(kind), at]
        step = (1 - 2 * way) * (s + 1 if self.direct else 1)
        return pltpu.make_async_remote_copy(
            src_ref=c, dst_ref=c, send_sem=self.send.at[kind, 0], recv_sem=self.near.at[kind, way, s],
            device_id=self.device(kind == 0, step), device_id_type=MESH)

    def far_copy(self, kind, way, s, at2, at1):
        if self.group == 1:
            c = self.arrays[kind].at[at2, at1]
        else:
            c = self.arrays[kind].at[at2, pl.ds(2 * at1, 2)]
        return pltpu.make_async_remote_copy(
            src_ref=c, dst_ref=c, send_sem=self.send.at[kind, 1], recv_sem=self.far.at[kind, way, s, at1],
            device_id=self.device(kind == 1, 1 - 2 * way), device_id_type=MESH)

    def place(self, kind, j):
        me = self.me1(kind)
        if self.group == 1:
            half = lax.div(j + 1, 2)
            return wrap(me + half * (1 - 2 * lax.rem(j, 2)))
        pair, side = lax.div(me, 2), 1 - 2 * lax.rem(me, 2)
        offset = (0, -side, side, 2)[j]
        return lax.rem(pair + offset + 4, 4)

    def open_chunk(self, j):
        for kind in range(2):
            for way in range(2):
                self.far_copy(kind, way, 0, self.me2(kind), self.place(kind, j)).start()

    def begin(self):
        for s in range(4 if self.direct else 1):
            for kind in range(2):
                for way in range(2 if s < 3 else 1):
                    self.near_copy(kind, way, s, self.me1(kind)).start()
        if self.group == 1:
            self.open_chunk(0)

    def near_step(self, u):
        for way in range(2 if u < 4 else 1):
            for kind in range(2):
                at = wrap(self.me1(kind) - u * (1 - 2 * way))
                self.near_copy(kind, way, u - 1, at).wait_recv()
                if u < 4 - way and not self.direct:
                    self.near_copy(kind, way, u, at).start()
        if self.group == 1:
            self.open_chunk(2 * u - 1)
            if u < 4:
                self.open_chunk(2 * u)
        else:
            self.open_chunk(u - 1)

    def far_step(self, s, j):
        for way in range(2):
            mine = lax.rem(jnp.int32(j), 2) == way
            for kind in range(2):
                at1 = self.place(kind, j)
                at2 = wrap(self.me2(kind) - s * (1 - 2 * way))

                def arrive():
                    self.far_copy(kind, way, s - 1, at2, at1).wait_recv()

                def forward():
                    self.far_copy(kind, way, s, at2, at1).start()

                if isinstance(j, int):
                    if s < 4 or j % 2 == way:
                        arrive()
                    if s < 3 or (s == 3 and j % 2 == way):
                        forward()
                    continue
                if s < 4:
                    arrive()
                else:
                    pl.when(mine)(arrive)
                if s < 3:
                    forward()
                elif s == 3:
                    pl.when(mine)(forward)

    def far_steps(self, s):
        @pl.loop(0, 8 // self.group)
        def _(j):
            self.far_step(s, j)

    def finish(self):
        for kind in range(2):
            for i, part in enumerate((self.arrays[kind].at[0, 0:7], self.arrays[kind].at[0:7])):
                pltpu.make_async_remote_copy(
                    src_ref=part, dst_ref=part, send_sem=self.send.at[kind, i],
                    recv_sem=self.near.at[kind, 0, 0],
                    device_id=self.device(True, 1), device_id_type=MESH).wait_send()


def kernel(
    lam_ref, hgain_ref, ngain_ref, res_hbm, q_hbm, key_hbm, val_hbm, ow_hbm, up_hbm, down_hbm,
    out_ref,
    kv_a, kv_b, up_a, up_b, dn_a, dn_b, res_ref, ow_ref, q_all, st_all, ho_all, an_all, sq_all,
    pre_out, pre_in, rs_out, rs_all, keep, o_scr, mix_a, mix_b, got_a, got_b,
    kv_send, kv_near, kv_far, u_send, u_near, u_far, d_send, d_near, d_far,
    x_send, x_recv, pre_send, pre_recv, in_sem,
):
    sp, tp = lax.axis_index("sp"), lax.axis_index("tp")
    z, y = lax.div(sp, RING), lax.rem(sp, RING)
    x, c = lax.div(tp, 2), lax.rem(tp, 2)
    partner = x * 2 + 1 - c
    kv = Gather(kv_a, kv_b, y, z, tp, (kv_send, kv_near, kv_far), True, 1)
    w1 = Gather(up_a, up_b, y, z, tp, (u_send, u_near, u_far), False, 2)
    w2 = Gather(dn_a, dn_b, y, z, tp, (d_send, d_near, d_far), False, 2)

    barrier = pltpu.get_barrier_semaphore()

    @pl.loop(1, RING)
    def _(p):
        pl.semaphore_signal(barrier, inc=1, device_id=(sp, wrap(tp + p)), device_id_type=MESH)
        for along_y in (True, False):
            pl.semaphore_signal(barrier, inc=1, device_id=kv.device(along_y, p), device_id_type=MESH)

    loads = [
        pltpu.make_async_copy(src, dst, in_sem.at[i])
        for i, (src, dst) in enumerate((
            (key_hbm.at[:, 0:256], kv_a.at[z, y, :, 0:256]),
            (val_hbm.at[:, 0:256], kv_a.at[z, y, :, 256:512]),
            (key_hbm.at[:, 256:512], kv_b.at[y, z, :, 0:256]),
            (val_hbm.at[:, 256:512], kv_b.at[y, z, :, 256:512]),
            (q_hbm, q_all.at[tp]),
            (up_hbm.at[:, 0:512], up_a.at[z, y]),
            (up_hbm.at[:, 512:1024], up_b.at[y, z]),
            (down_hbm.at[0:16], dn_a.at[z, y]),
            (down_hbm.at[16:32], dn_b.at[y, z]),
            (res_hbm, res_ref),
            (ow_hbm, ow_ref),
        ))
    ]
    for load in loads:
        load.start()
    for load in loads:
        load.wait()
    pl.semaphore_wait(barrier, TP - 1 + 2 * (RING - 1))

    def chip(step):
        return lax.rem(x + step + 4, 4)

    def tp_of(step):
        return chip(step) * 2 + c

    def x_copy(k, src, dst, slot, peer):
        return pltpu.make_async_remote_copy(
            src_ref=src, dst_ref=dst.at[slot], send_sem=x_send.at[k], recv_sem=x_recv.at[k, slot],
            device_id=(sp, peer), device_id_type=MESH)

    def x_arrived(k, dst, slot):
        x_copy(k, dst.at[slot], dst, slot, partner).wait_recv()

    def share(k, array):
        for step in (2, 1, 3):
            x_copy(k, array.at[tp], array, tp, tp_of(step)).start()
        x_copy(k, array.at[tp], array, tp, partner).start()

    def relay(k, array):
        for step in (1, 3, 2):
            slot = tp_of(step)
            x_arrived(k, array, slot)
            x_copy(k, array.at[slot], array, slot, partner).start()

    def collect(k, array):
        for step in (0, 1, 3, 2):
            x_arrived(k, array, chip(step) * 2 + 1 - c)

    def x_sent(k, part):
        pltpu.make_async_remote_copy(
            src_ref=part, dst_ref=part, send_sem=x_send.at[k], recv_sem=x_recv.at[k, 0],
            device_id=(sp, partner), device_id_type=MESH).wait_send()

    events = [(w1, 1, j) for j in range(4)]
    for j in range(4):
        events += [(w2, 0, j + 1), (w1, 2, j)]
    for j in range(4):
        events += [(w1, 3, j), (w2, 1, j)]
    for j in range(4):
        events += [(w1, 4, j), (w2, 2, j)]

    def pump(count):
        for _ in range(count):
            gather, s, j = events.pop(0)
            if s == 0:
                gather.near_step(j)
            else:
                gather.far_step(s, j)

    kv.begin()
    share(0, q_all)
    w1.begin()
    for u in range(1, 5):
        kv.near_step(u)
    relay(0, q_all)
    for s in range(1, 4):
        kv.far_steps(s)
        w1.near_step(s)
    w1.near_step(4)
    w2.begin()
    kv.far_steps(4)
    collect(0, q_all)

    lane = lax.broadcasted_iota(jnp.int32, (ROWS, 128), 1)
    stats = jnp.zeros((ROWS, 128), F32)
    for gc in range(4):
        g, m_c = gc // 2, gc % 2
        whole = kv_a if g == 0 else kv_b
        q = q_all[4 * g : 4 * g + 4, :, m_c * 128 : m_c * 128 + 128].reshape(4 * ROWS, 128)
        k = whole[:, :, :, m_c * 128 : m_c * 128 + 128].reshape(1024, 128)
        v = whole[:, :, :, 256:512].reshape(1024, 256)
        s = lax.dot_general(q, k, NT, preferred_element_type=F32)
        m = jnp.max(s, axis=1, keepdims=True)
        p = jnp.exp2((s - m) * LOG_SCALE)
        t = jnp.sum(p, axis=1, keepdims=True)
        o = jnp.dot(p.astype(BF16), v, preferred_element_type=F32)
        m = m * LOG_SCALE
        for i in range(4):
            at = (4 * g + i) * 2 + m_c
            o_scr[at] = o[i * ROWS : (i + 1) * ROWS]
            stats = jnp.where(lane == at, m[i * ROWS : (i + 1) * ROWS], stats)
            stats = jnp.where(lane == at + 16, t[i * ROWS : (i + 1) * ROWS], stats)
        pump(1)

    st_all[tp] = jnp.transpose(stats)[0:32]
    pump(1)
    for step in (2, 1, 3):
        for core in range(2):
            x_copy(1, st_all.at[tp], st_all, tp, chip(step) * 2 + core).start()
    x_copy(1, st_all.at[tp], st_all, tp, partner).start()
    pump(2)
    x_arrived(1, st_all, partner)
    for step in (1, 3, 2):
        for core in range(2):
            x_arrived(1, st_all, chip(step) * 2 + core)

    every = st_all[...]
    maxima, totals = every[:, 0:16], every[:, 16:32]
    highest = jnp.max(maxima, axis=0)
    total = jnp.sum(jnp.exp2(maxima - highest[None]) * totals, axis=0)
    mine = st_all[tp]
    coef = jnp.exp2(mine[0:16] - highest) / total
    row = lax.broadcasted_iota(jnp.int32, (16, 128), 0)
    factor = jnp.ones((16, 128), F32)
    for h in range(HEADS):
        factor = jnp.where(row == 2 * h + 1, -lam_ref[h], factor)
    coef = jnp.concatenate([coef * factor, jnp.zeros((112, 128), F32)], axis=0)
    coef = jnp.transpose(coef)

    def differ(i, h):
        even = lax.rem(h, 2) == 0
        first = jnp.where(even, coef[:, 4 * i : 4 * i + 1], coef[:, 4 * i + 2 : 4 * i + 3])
        second = jnp.where(even, coef[:, 4 * i + 1 : 4 * i + 2], coef[:, 4 * i + 3 : 4 * i + 4])
        return o_scr[2 * h] * first + o_scr[2 * h + 1] * second

    for i in range(4):
        pre_out[i] = differ(i, 2 * i + 1 - c).astype(BF16)
    across = pltpu.make_async_remote_copy(
        src_ref=pre_out, dst_ref=pre_in, send_sem=pre_send, recv_sem=pre_recv,
        device_id=(sp, partner), device_id_type=MESH)
    across.start()
    for i in range(4):
        keep[i] = differ(i, 2 * i + c)
    across.wait_recv()
    for step in (2, 1, 3):
        i = chip(step)
        rs_out[i] = (keep[i] + pre_in[i].astype(F32)).astype(BF16)
    for step in (2, 1, 3):
        i = chip(step)
        x_copy(2, rs_out.at[i], rs_all, x, tp_of(step)).start()
    difference = keep[x] + pre_in[x].astype(F32)
    pump(5)
    for step in (1, 3, 2):
        i = chip(step)
        x_arrived(2, rs_all, i)
        difference += rs_all[i].astype(F32)

    square = jnp.mean(difference * difference, axis=-1, keepdims=True)
    ho_all[tp] = (difference * lax.rsqrt(square + EPSILON) * hgain_ref[...]).astype(BF16)
    pump(1)
    share(3, ho_all)
    pump(4)
    relay(3, ho_all)
    pump(1)
    collect(3, ho_all)
    heads = jnp.concatenate([ho_all[h] for h in range(HEADS)], axis=1)
    projected = jnp.dot(heads, ow_ref[...], preferred_element_type=F32)
    after_mix = res_ref[...].astype(F32) + projected
    keep[0] = after_mix
    an_all[tp] = (after_mix * ngain_ref[...]).astype(BF16)
    squares = jnp.sum(after_mix * after_mix, axis=1, keepdims=True)
    sq_all[tp] = jnp.transpose(jnp.broadcast_to(squares, (ROWS, 128)))[0:8]
    pump(1)
    share(4, an_all)
    share(5, sq_all)
    pump(4)
    relay(4, an_all)
    relay(5, sq_all)
    pump(1)
    collect(4, an_all)
    collect(5, sq_all)
    squares = jnp.sum(sq_all[...], axis=0)
    squares = jnp.transpose(jnp.broadcast_to(squares[0:1], (128, 128)))[:, 0:1]
    scale = lax.rsqrt(squares / D + EPSILON)
    pump(len(events))

    normed = jnp.concatenate([an_all[t] for t in range(TP)], axis=1)
    parts = []
    for half in range(2):
        if half == 0:
            weights = up_a[...].reshape(2048, 512)
        else:
            weights = jnp.concatenate([up_b[:, t].reshape(256, 512) for t in range(TP)], axis=0)
        hidden = jnp.dot(normed, weights, preferred_element_type=F32) * scale
        parts.append(jnp.square(jax.nn.relu(hidden)).astype(BF16))
    activated = jnp.concatenate(parts, axis=1)

    def mix(weights):
        return lax.dot_general(
            activated, weights.reshape(128, 1024), NT, preferred_element_type=F32).astype(BF16)

    def give(k, out, got, t):
        @pl.when(t != tp)
        def _():
            x_copy(k, out.at[t], got, tp, t).start()

        @pl.when(t == tp)
        def _():
            got[tp] = out[tp]

    def give_a(places):
        for t in places:
            mix_a[t] = mix(dn_a[t])
        for t in places:
            give(6, mix_a, got_a, t)

    give_a([z])
    give_a([wrap(z + 1), wrap(z - 1)])
    give_a([wrap(z + 2), wrap(z - 2)])
    for j in range(4):
        w2.far_step(3, j)
    give_a([wrap(z + 3), wrap(z - 3)])
    for j in range(4):
        w2.far_step(4, j)

    order = [chip(step) * 2 + core for step in (2, 1, 3, 0) for core in range(2)]
    for n, t in enumerate(order):
        mix_b[t] = mix(dn_b[:, t])
        if n > 0:
            give(7, mix_b, got_b, order[n - 1])
    give(7, mix_b, got_b, order[-1])
    give_a([wrap(z + 4)])

    def spread(got, shift):
        source = lax.broadcasted_iota(jnp.int32, (128, 256), 0)
        target = lax.broadcasted_iota(jnp.int32, (128, 256), 1)
        at = lax.div(source, 16) * 32 + lax.rem(source, 16) + shift
        matrix = jnp.where(at == target, 1.0, 0.0).astype(BF16)
        rows = jnp.concatenate([got[t] for t in range(TP)], axis=1)
        return jnp.dot(rows, jnp.concatenate([matrix] * TP, axis=0), preferred_element_type=F32)

    for k, got in ((6, got_a), (7, got_b)):
        @pl.loop(1, TP)
        def _(p):
            x_arrived(k, got, wrap(tp - p))

    out_ref[...] = (keep[0] + (spread(got_a, 0) + spread(got_b, 16))).astype(BF16)

    kv.finish()
    w1.finish()
    w2.finish()
    for k, array in ((0, q_all), (1, st_all), (3, ho_all), (4, an_all), (5, sq_all), (6, mix_a), (7, mix_b)):
        x_sent(k, array.at[0:7])
    x_sent(2, rs_out.at[0:3])
    across.wait_send()


def on_device(residual, queries, key_proj, value_proj, diff_lambda, head_gain, out_weight, norm_gain, up_weight, down_weight):
    vmem = pl.BlockSpec(memory_space=pltpu.VMEM)
    smem = pl.BlockSpec(memory_space=pltpu.SMEM)
    hbm = pl.BlockSpec(memory_space=pltpu.HBM)
    block = (TP, ROWS, 256)
    half = (TP, ROWS, 128)
    dma = pltpu.SemaphoreType.DMA
    return pl.pallas_call(
        kernel,
        out_shape=jax.ShapeDtypeStruct((ROWS, 256), BF16),
        in_specs=[smem, vmem, vmem] + [hbm] * 7,
        out_specs=vmem,
        scratch_shapes=[
            pltpu.VMEM((RING, RING, 16, 512), BF16),
            pltpu.VMEM((RING, RING, 16, 512), BF16),
            pltpu.VMEM((RING, RING, 32, 512), BF16),
            pltpu.VMEM((RING, RING, 32, 512), BF16),
            pltpu.VMEM((RING, RING, 16, 1024), BF16),
            pltpu.VMEM((RING, RING, 16, 1024), BF16),
            pltpu.VMEM((ROWS, 256), BF16),
            pltpu.VMEM((2048, 256), BF16),
            pltpu.VMEM(block, BF16),
            pltpu.VMEM((TP, 32, 128), F32),
            pltpu.VMEM(block, BF16),
            pltpu.VMEM(block, BF16),
            pltpu.VMEM((TP, 8, 128), F32),
            pltpu.VMEM((4, ROWS, 256), BF16),
            pltpu.VMEM((4, ROWS, 256), BF16),
            pltpu.VMEM((4, ROWS, 256), BF16),
            pltpu.VMEM((4, ROWS, 256), BF16),
            pltpu.VMEM((4, ROWS, 256), F32),
            pltpu.VMEM((16, ROWS, 256), F32),
            pltpu.VMEM(half, BF16),
            pltpu.VMEM(half, BF16),
            pltpu.VMEM(half, BF16),
            pltpu.VMEM(half, BF16),
            dma((2, 2)), dma((2, 2, 4)), dma((2, 2, 4, 8)),
            dma((2, 2)), dma((2, 2, 4)), dma((2, 2, 4, 4)),
            dma((2, 2)), dma((2, 2, 4)), dma((2, 2, 4, 4)),
            dma((8,)), dma((8, TP)), dma, dma, dma((11,)),
        ],
        compiler_params=pltpu.CompilerParams(
            collective_id=0, has_side_effects=True, vmem_limit_bytes=67043328),
    )(diff_lambda, head_gain.reshape(1, 256), norm_gain.reshape(1, 256), residual, queries, key_proj, value_proj,
      out_weight, up_weight, down_weight.T)


def solution(mesh):
    return jax.shard_map(
        on_device,
        mesh=mesh,
        in_specs=(
            P("sp", "tp"),
            P("sp", "tp"),
            P(("sp", "tp"), None),
            P(("sp", "tp"), None),
            P(),
            P(),
            P(None, "tp"),
            P("tp"),
            P("sp", "tp"),
            P("tp", "sp"),
        ),
        out_specs=P("sp", "tp"),
        check_vma=False,
    )
```

```python
import jax
import jax.numpy as jnp
from jax import lax
from jax.experimental import pallas as pl
from jax.experimental.pallas import tpu as pltpu
from jax.sharding import PartitionSpec as P

D = 2048
HEADS = 8
HEAD_DIM = 128
RING = 8
TP = 8
ROWS = 128
EPSILON = 1e-06
MESH = pl.DeviceIdType.MESH
F32 = jnp.float32
BF16 = jnp.bfloat16
LOG_SCALE = HEAD_DIM ** (-0.5) * 1.4426950408889634
NT = (((1,), (1,)), ((), ()))


def wrap(i):
    return lax.rem(i + RING, RING)


class Gather:
    def __init__(self, first, second, y, z, tp, sems, direct):
        self.arrays = (first, second)
        self.y, self.z, self.tp = y, z, tp
        self.send, self.near, self.far = sems
        self.direct = direct

    def me1(self, kind):
        return self.y if kind == 0 else self.z

    def me2(self, kind):
        return self.z if kind == 0 else self.y

    def device(self, along_y, step):
        if along_y:
            return (self.z * RING + wrap(self.y + step), self.tp)
        return (wrap(self.z + step) * RING + self.y, self.tp)

    def near_copy(self, kind, way, s, at):
        c = self.arrays[kind].at[self.me2(kind), at]
        step = (1 - 2 * way) * (s + 1 if self.direct else 1)
        return pltpu.make_async_remote_copy(
            src_ref=c, dst_ref=c, send_sem=self.send.at[kind, 0], recv_sem=self.near.at[kind, way, s],
            device_id=self.device(kind == 0, step), device_id_type=MESH)

    def far_copy(self, kind, way, s, at2, at1):
        c = self.arrays[kind].at[at2, pl.ds(2 * at1, 2)]
        return pltpu.make_async_remote_copy(
            src_ref=c, dst_ref=c, send_sem=self.send.at[kind, 1], recv_sem=self.far.at[kind, way, s, at1],
            device_id=self.device(kind == 1, 1 - 2 * way), device_id_type=MESH)

    def place(self, kind, j):
        me = self.me1(kind)
        pair, side = lax.div(me, 2), 1 - 2 * lax.rem(me, 2)
        offset = (0, -side, side, 2)[j]
        return lax.rem(pair + offset + 4, 4)

    def open_chunk(self, j):
        for kind in range(2):
            for way in range(2):
                self.far_copy(kind, way, 0, self.me2(kind), self.place(kind, j)).start()

    def begin(self):
        for s in range(4 if self.direct else 1):
            for kind in range(2):
                for way in range(2 if s < 3 else 1):
                    self.near_copy(kind, way, s, self.me1(kind)).start()

    def near_step(self, u):
        for way in range(2 if u < 4 else 1):
            for kind in range(2):
                at = wrap(self.me1(kind) - u * (1 - 2 * way))
                self.near_copy(kind, way, u - 1, at).wait_recv()
                if u < 4 - way and not self.direct:
                    self.near_copy(kind, way, u, at).start()
        self.open_chunk(u - 1)

    def far_step(self, s, j):
        for way in range(2):
            for kind in range(2):
                at1 = self.place(kind, j)
                at2 = wrap(self.me2(kind) - s * (1 - 2 * way))
                if s < 4 or j % 2 == way:
                    self.far_copy(kind, way, s - 1, at2, at1).wait_recv()
                if s < 3 or (s == 3 and j % 2 == way):
                    self.far_copy(kind, way, s, at2, at1).start()

    def far_steps(self, s):
        for j in range(4):
            self.far_step(s, j)

    def finish(self):
        for kind in range(2):
            for i, part in enumerate((self.arrays[kind].at[0, 0:7], self.arrays[kind].at[0:7])):
                pltpu.make_async_remote_copy(
                    src_ref=part, dst_ref=part, send_sem=self.send.at[kind, i],
                    recv_sem=self.near.at[kind, 0, 0],
                    device_id=self.device(True, 1), device_id_type=MESH).wait_send()


def kernel(
    lam_ref, hgain_ref, ngain_ref, res_hbm, q_hbm, key_hbm, val_hbm, ow_hbm, up_hbm, down_hbm,
    out_ref,
    kv_a, kv_b, up_a, up_b, dn_a, dn_b, res_ref, ow_ref, q_all, st_all, ho_all, an_all, sq_all,
    pre_out, pre_in, rs_out, rs_all, keep, o_scr, mix_a, mix_b, got_a, got_b,
    kv_send, kv_near, kv_far, u_send, u_near, u_far, d_send, d_near, d_far,
    x_send, x_recv, pre_send, pre_recv, in_sem,
):
    sp, tp = lax.axis_index("sp"), lax.axis_index("tp")
    z, y = lax.div(sp, RING), lax.rem(sp, RING)
    x, c = lax.div(tp, 2), lax.rem(tp, 2)
    partner = x * 2 + 1 - c
    kv = Gather(kv_a, kv_b, y, z, tp, (kv_send, kv_near, kv_far), True)
    w1 = Gather(up_a, up_b, y, z, tp, (u_send, u_near, u_far), False)
    w2 = Gather(dn_a, dn_b, y, z, tp, (d_send, d_near, d_far), False)

    barrier = pltpu.get_barrier_semaphore()

    @pl.loop(1, RING)
    def _(p):
        pl.semaphore_signal(barrier, inc=1, device_id=(sp, wrap(tp + p)), device_id_type=MESH)
        for along_y in (True, False):
            pl.semaphore_signal(barrier, inc=1, device_id=kv.device(along_y, p), device_id_type=MESH)

    loads = [
        pltpu.make_async_copy(src, dst, in_sem.at[i])
        for i, (src, dst) in enumerate((
            (key_hbm.at[:, 0:256], kv_a.at[z, y, :, 0:256]),
            (val_hbm.at[:, 0:256], kv_a.at[z, y, :, 256:512]),
            (key_hbm.at[:, 256:512], kv_b.at[y, z, :, 0:256]),
            (val_hbm.at[:, 256:512], kv_b.at[y, z, :, 256:512]),
            (q_hbm, q_all.at[tp]),
            (up_hbm.at[:, 0:512], up_a.at[z, y]),
            (up_hbm.at[:, 512:1024], up_b.at[y, z]),
            (down_hbm.at[0:16], dn_a.at[z, y]),
            (down_hbm.at[16:32], dn_b.at[y, z]),
            (res_hbm, res_ref),
            (ow_hbm, ow_ref),
        ))
    ]
    for load in loads:
        load.start()
    for load in loads:
        load.wait()
    pl.semaphore_wait(barrier, TP - 1 + 2 * (RING - 1))

    def chip(step):
        return lax.rem(x + step + 4, 4)

    def tp_of(step):
        return chip(step) * 2 + c

    def x_copy(k, src, dst, slot, peer):
        return pltpu.make_async_remote_copy(
            src_ref=src, dst_ref=dst.at[slot], send_sem=x_send.at[k], recv_sem=x_recv.at[k, slot],
            device_id=(sp, peer), device_id_type=MESH)

    def x_arrived(k, dst, slot):
        x_copy(k, dst.at[slot], dst, slot, partner).wait_recv()

    def share(k, array):
        for step in (2, 1, 3):
            x_copy(k, array.at[tp], array, tp, tp_of(step)).start()
        x_copy(k, array.at[tp], array, tp, partner).start()

    def relay(k, array):
        for step in (1, 3, 2):
            slot = tp_of(step)
            x_arrived(k, array, slot)
            x_copy(k, array.at[slot], array, slot, partner).start()

    def collect(k, array):
        for step in (0, 1, 3, 2):
            x_arrived(k, array, chip(step) * 2 + 1 - c)

    def x_sent(k, part):
        pltpu.make_async_remote_copy(
            src_ref=part, dst_ref=part, send_sem=x_send.at[k], recv_sem=x_recv.at[k, 0],
            device_id=(sp, partner), device_id_type=MESH).wait_send()

    events = [(w1, 1, j) for j in range(4)]
    for j in range(4):
        events += [(w2, 0, j + 1), (w1, 2, j)]
    for j in range(4):
        events += [(w1, 3, j), (w2, 1, j)]
    for j in range(4):
        events += [(w1, 4, j), (w2, 2, j)]

    def pump(count):
        for _ in range(count):
            gather, s, j = events.pop(0)
            if s == 0:
                gather.near_step(j)
            else:
                gather.far_step(s, j)

    kv.begin()
    share(0, q_all)
    w1.begin()
    for u in range(1, 5):
        kv.near_step(u)
    relay(0, q_all)
    for s in range(1, 4):
        kv.far_steps(s)
        w1.near_step(s)
    w1.near_step(4)
    w2.begin()
    kv.far_steps(4)
    collect(0, q_all)

    lane = lax.broadcasted_iota(jnp.int32, (ROWS, 128), 1)
    stats = jnp.zeros((ROWS, 128), F32)
    for gc in range(4):
        g, m_c = gc // 2, gc % 2
        whole = kv_a if g == 0 else kv_b
        q = q_all[4 * g : 4 * g + 4, :, m_c * 128 : m_c * 128 + 128].reshape(4 * ROWS, 128)
        k = whole[:, :, :, m_c * 128 : m_c * 128 + 128].reshape(1024, 128)
        v = whole[:, :, :, 256:512].reshape(1024, 256)
        s = lax.dot_general(q, k, NT, preferred_element_type=F32)
        m = jnp.max(s, axis=1, keepdims=True)
        p = jnp.exp2((s - m) * LOG_SCALE)
        t = jnp.sum(p, axis=1, keepdims=True)
        o = jnp.dot(p.astype(BF16), v, preferred_element_type=F32)
        m = m * LOG_SCALE
        for i in range(4):
            at = (4 * g + i) * 2 + m_c
            o_scr[at] = o[i * ROWS : (i + 1) * ROWS]
            stats = jnp.where(lane == at, m[i * ROWS : (i + 1) * ROWS], stats)
            stats = jnp.where(lane == at + 16, t[i * ROWS : (i + 1) * ROWS], stats)
        pump(1)

    st_all[tp] = jnp.transpose(stats)[0:32]
    pump(1)
    for step in (2, 1, 3):
        for core in range(2):
            x_copy(1, st_all.at[tp], st_all, tp, chip(step) * 2 + core).start()
    x_copy(1, st_all.at[tp], st_all, tp, partner).start()
    pump(3)
    x_arrived(1, st_all, partner)
    for step in (1, 3, 2):
        for core in range(2):
            x_arrived(1, st_all, chip(step) * 2 + core)

    every = st_all[...]
    maxima, totals = every[:, 0:16], every[:, 16:32]
    highest = jnp.max(maxima, axis=0)
    total = jnp.sum(jnp.exp2(maxima - highest[None]) * totals, axis=0)
    mine = st_all[tp]
    coef = jnp.exp2(mine[0:16] - highest) / total
    row = lax.broadcasted_iota(jnp.int32, (16, 128), 0)
    factor = jnp.ones((16, 128), F32)
    for h in range(HEADS):
        factor = jnp.where(row == 2 * h + 1, -lam_ref[h], factor)
    coef = jnp.concatenate([coef * factor, jnp.zeros((112, 128), F32)], axis=0)
    coef = jnp.transpose(coef)

    def differ(i, h):
        even = lax.rem(h, 2) == 0
        first = jnp.where(even, coef[:, 4 * i : 4 * i + 1], coef[:, 4 * i + 2 : 4 * i + 3])
        second = jnp.where(even, coef[:, 4 * i + 1 : 4 * i + 2], coef[:, 4 * i + 3 : 4 * i + 4])
        return o_scr[2 * h] * first + o_scr[2 * h + 1] * second

    for i in range(4):
        pre_out[i] = differ(i, 2 * i + 1 - c).astype(BF16)
    across = pltpu.make_async_remote_copy(
        src_ref=pre_out, dst_ref=pre_in, send_sem=pre_send, recv_sem=pre_recv,
        device_id=(sp, partner), device_id_type=MESH)
    across.start()
    pump(1)
    for i in range(4):
        keep[i] = differ(i, 2 * i + c)
    pump(1)
    across.wait_recv()
    for step in (2, 1, 3):
        i = chip(step)
        rs_out[i] = (keep[i] + pre_in[i].astype(F32)).astype(BF16)
    for step in (2, 1, 3):
        i = chip(step)
        x_copy(2, rs_out.at[i], rs_all, x, tp_of(step)).start()
    difference = keep[x] + pre_in[x].astype(F32)
    pump(5)
    for step in (1, 3, 2):
        i = chip(step)
        x_arrived(2, rs_all, i)
        difference += rs_all[i].astype(F32)

    square = jnp.mean(difference * difference, axis=-1, keepdims=True)
    ho_all[tp] = (difference * lax.rsqrt(square + EPSILON) * hgain_ref[...]).astype(BF16)
    pump(1)
    share(3, ho_all)
    pump(3)
    relay(3, ho_all)
    pump(1)
    collect(3, ho_all)
    heads = jnp.concatenate([ho_all[h] for h in range(HEADS)], axis=1)
    projected = jnp.dot(heads, ow_ref[...], preferred_element_type=F32)
    after_mix = res_ref[...].astype(F32) + projected
    keep[0] = after_mix
    an_all[tp] = (after_mix * ngain_ref[...]).astype(BF16)
    squares = jnp.sum(after_mix * after_mix, axis=1, keepdims=True)
    sq_all[tp] = jnp.transpose(jnp.broadcast_to(squares, (ROWS, 128)))[0:8]
    pump(1)
    share(4, an_all)
    share(5, sq_all)
    pump(4)
    relay(4, an_all)
    relay(5, sq_all)
    pump(1)
    collect(4, an_all)
    collect(5, sq_all)
    squares = jnp.sum(sq_all[...], axis=0)
    squares = jnp.transpose(jnp.broadcast_to(squares[0:1], (128, 128)))[:, 0:1]
    scale = lax.rsqrt(squares / D + EPSILON)
    pump(len(events))

    normed = jnp.concatenate([an_all[t] for t in range(TP)], axis=1)
    parts = []
    for half in range(2):
        if half == 0:
            weights = up_a[...].reshape(2048, 512)
        else:
            weights = jnp.concatenate([up_b[:, t].reshape(256, 512) for t in range(TP)], axis=0)
        hidden = jnp.dot(normed, weights, preferred_element_type=F32) * scale
        parts.append(jnp.square(jax.nn.relu(hidden)).astype(BF16))
    activated = jnp.concatenate(parts, axis=1)

    def mix(weights):
        return lax.dot_general(
            activated, weights.reshape(128, 1024), NT, preferred_element_type=F32).astype(BF16)

    def give(k, out, got, t):
        @pl.when(t != tp)
        def _():
            x_copy(k, out.at[t], got, tp, t).start()

        @pl.when(t == tp)
        def _():
            got[tp] = out[tp]

    def give_a(places):
        for t in places:
            mix_a[t] = mix(dn_a[t])
        for t in places:
            give(6, mix_a, got_a, t)

    def mix_block(d):
        block = dn_b[wrap(y + offsets[d])].reshape(128, 1024)
        sums = lax.dot_general(block, activated, NT, preferred_element_type=F32)
        mix_b[:, d] = sums.astype(BF16).reshape(TP, 16, 128)

    def b_copy(k, t, part):
        return pltpu.make_async_remote_copy(
            src_ref=mix_b.at[t, part], dst_ref=got_b.at[tp, part], send_sem=x_send.at[k],
            recv_sem=x_recv.at[k, tp], device_id=(sp, t), device_id_type=MESH)

    def give_b(k, part):
        for step in (2, 1, 3):
            for core in range(2):
                b_copy(k, chip(step) * 2 + core, part).start()
        b_copy(k, partner, part).start()

    def got_part(k, part):
        @pl.loop(1, TP)
        def _(p):
            slot = wrap(tp - p)
            there = got_b.at[slot, part]
            pltpu.make_async_remote_copy(
                src_ref=there, dst_ref=there, send_sem=x_send.at[k], recv_sem=x_recv.at[k, slot],
                device_id=(sp, partner), device_id_type=MESH).wait_recv()

    offsets = (0, 1, -1, 2, -2, 3, -3, 4)
    early, late = pl.ds(0, 7), pl.ds(7, 1)
    give_a([z])
    give_a([wrap(z + 1), wrap(z - 1)])
    for d in range(3):
        mix_block(d)
    give_a([wrap(z + 2), wrap(z - 2)])
    for d in range(3, 5):
        mix_block(d)
    for j in range(4):
        w2.far_step(3, j)
    give_a([wrap(z + 3), wrap(z - 3)])
    for d in range(5, 7):
        mix_block(d)
    give_b(7, early)
    for j in range(4):
        w2.far_step(4, j)
    mix_block(7)
    give_a([wrap(z + 4)])
    give_b(8, late)
    got_b[tp] = mix_b[tp]

    @pl.loop(1, TP)
    def _(p):
        x_arrived(6, got_a, wrap(tp - p))

    source = lax.broadcasted_iota(jnp.int32, (128, 256), 0)
    target = lax.broadcasted_iota(jnp.int32, (128, 256), 1)
    at = lax.div(source, 16) * 32 + lax.rem(source, 16)
    spread = jnp.where(at == target, 1.0, 0.0).astype(BF16)
    rows = jnp.concatenate([got_a[t] for t in range(TP)], axis=1)
    total = jnp.dot(rows, jnp.concatenate([spread] * TP, axis=0), preferred_element_type=F32)
    keep[0] = keep[0] + total

    target = lax.broadcasted_iota(jnp.int32, (256, 128), 0)
    source = lax.broadcasted_iota(jnp.int32, (256, 128), 1)
    d = lax.div(source, 16)
    at = y + lax.div(d + 1, 2) * (2 * lax.rem(d, 2) - 1)
    at = lax.rem(at + RING, RING) * 32 + 16 + lax.rem(source, 16)
    spread = jnp.where(at == target, 1.0, 0.0).astype(BF16)
    got_part(7, early)
    got_part(8, late)
    total = jnp.dot(
        jnp.concatenate([spread] * TP, axis=1), got_b[...].reshape(TP * 128, 128), preferred_element_type=F32)
    out_ref[...] = (keep[0] + jnp.transpose(total)).astype(BF16)

    kv.finish()
    w1.finish()
    w2.finish()
    for k, array in ((0, q_all), (1, st_all), (3, ho_all), (4, an_all), (5, sq_all), (6, mix_a)):
        x_sent(k, array.at[0:7])
    x_sent(2, rs_out.at[0:3])
    x_sent(7, mix_b.at[0:7, 0:7])
    x_sent(8, mix_b.at[0, 0:7])
    across.wait_send()


def on_device(residual, queries, key_proj, value_proj, diff_lambda, head_gain, out_weight, norm_gain, up_weight, down_weight):
    vmem = pl.BlockSpec(memory_space=pltpu.VMEM)
    smem = pl.BlockSpec(memory_space=pltpu.SMEM)
    hbm = pl.BlockSpec(memory_space=pltpu.HBM)
    block = (TP, ROWS, 256)
    half = (TP, ROWS, 128)
    dma = pltpu.SemaphoreType.DMA
    return pl.pallas_call(
        kernel,
        out_shape=jax.ShapeDtypeStruct((ROWS, 256), BF16),
        in_specs=[smem, vmem, vmem] + [hbm] * 7,
        out_specs=vmem,
        scratch_shapes=[
            pltpu.VMEM((RING, RING, 16, 512), BF16),
            pltpu.VMEM((RING, RING, 16, 512), BF16),
            pltpu.VMEM((RING, RING, 32, 512), BF16),
            pltpu.VMEM((RING, RING, 32, 512), BF16),
            pltpu.VMEM((RING, RING, 16, 1024), BF16),
            pltpu.VMEM((RING, RING, 16, 1024), BF16),
            pltpu.VMEM((ROWS, 256), BF16),
            pltpu.VMEM((2048, 256), BF16),
            pltpu.VMEM(block, BF16),
            pltpu.VMEM((TP, 32, 128), F32),
            pltpu.VMEM(block, BF16),
            pltpu.VMEM(block, BF16),
            pltpu.VMEM((TP, 8, 128), F32),
            pltpu.VMEM((4, ROWS, 256), BF16),
            pltpu.VMEM((4, ROWS, 256), BF16),
            pltpu.VMEM((4, ROWS, 256), BF16),
            pltpu.VMEM((4, ROWS, 256), BF16),
            pltpu.VMEM((4, ROWS, 256), F32),
            pltpu.VMEM((16, ROWS, 256), F32),
            pltpu.VMEM(half, BF16),
            pltpu.VMEM((TP, 8, 16, 128), BF16),
            pltpu.VMEM(half, BF16),
            pltpu.VMEM((TP, 8, 16, 128), BF16),
            dma((2, 2)), dma((2, 2, 4)), dma((2, 2, 4, 4)),
            dma((2, 2)), dma((2, 2, 4)), dma((2, 2, 4, 4)),
            dma((2, 2)), dma((2, 2, 4)), dma((2, 2, 4, 4)),
            dma((9,)), dma((9, TP)), dma, dma, dma((11,)),
        ],
        compiler_params=pltpu.CompilerParams(
            collective_id=0, has_side_effects=True, vmem_limit_bytes=67043328),
    )(diff_lambda, head_gain.reshape(1, 256), norm_gain.reshape(1, 256), residual, queries, key_proj, value_proj,
      out_weight, up_weight, down_weight.T)


def solution(mesh):
    return jax.shard_map(
        on_device,
        mesh=mesh,
        in_specs=(
            P("sp", "tp"),
            P("sp", "tp"),
            P(("sp", "tp"), None),
            P(("sp", "tp"), None),
            P(),
            P(),
            P(None, "tp"),
            P("tp"),
            P("sp", "tp"),
            P("tp", "sp"),
        ),
        out_specs=P("sp", "tp"),
        check_vma=False,
    )
```

```python
import jax
import jax.numpy as jnp
from jax import lax
from jax.experimental import pallas as pl
from jax.experimental.pallas import tpu as pltpu
from jax.sharding import PartitionSpec as P

D = 2048
HEADS = 8
HEAD_DIM = 128
RING = 8
TP = 8
ROWS = 128
EPSILON = 1e-06
MESH = pl.DeviceIdType.MESH
F32 = jnp.float32
BF16 = jnp.bfloat16
LOG_SCALE = HEAD_DIM ** (-0.5) * 1.4426950408889634
NT = (((1,), (1,)), ((), ()))


def wrap(i):
    return lax.rem(i + RING, RING)


class Gather:
    def __init__(self, first, second, y, z, tp, sems, direct):
        self.arrays = (first, second)
        self.y, self.z, self.tp = y, z, tp
        self.send, self.near, self.far = sems
        self.direct = direct

    def me1(self, kind):
        return self.y if kind == 0 else self.z

    def me2(self, kind):
        return self.z if kind == 0 else self.y

    def device(self, along_y, step):
        if along_y:
            return (self.z * RING + wrap(self.y + step), self.tp)
        return (wrap(self.z + step) * RING + self.y, self.tp)

    def near_copy(self, kind, way, s, at):
        c = self.arrays[kind].at[self.me2(kind), at]
        step = (1 - 2 * way) * (s + 1 if self.direct else 1)
        return pltpu.make_async_remote_copy(
            src_ref=c, dst_ref=c, send_sem=self.send.at[kind, 0], recv_sem=self.near.at[s],
            device_id=self.device(kind == 0, step), device_id_type=MESH)

    def far_copy(self, kind, way, s, j, at2):
        c = self.arrays[kind].at[at2, pl.ds(2 * self.place(kind, j), 2)]
        return pltpu.make_async_remote_copy(
            src_ref=c, dst_ref=c, send_sem=self.send.at[kind, 1], recv_sem=self.far.at[s, j],
            device_id=self.device(kind == 1, 1 - 2 * way), device_id_type=MESH)

    def place(self, kind, j):
        me = self.me1(kind)
        pair, side = lax.div(me, 2), 1 - 2 * lax.rem(me, 2)
        offset = (0, -side, side, 2)[j]
        return lax.rem(pair + offset + 4, 4)

    def open_chunk(self, j):
        for kind in range(2):
            for way in range(2):
                self.far_copy(kind, way, 0, j, self.me2(kind)).start()

    def begin(self):
        for s in range(4 if self.direct else 1):
            for kind in range(2):
                for way in range(2 if s < 3 else 1):
                    self.near_copy(kind, way, s, self.me1(kind)).start()

    def arrived(self, sem, shards):
        part = self.arrays[0].at[0, 0:shards]
        pltpu.make_async_remote_copy(
            src_ref=part, dst_ref=part, send_sem=self.send.at[0, 0], recv_sem=sem,
            device_id=self.device(True, 1), device_id_type=MESH).wait_recv()

    def near_step(self, u):
        self.arrived(self.near.at[u - 1], 4 if u < 4 else 2)
        for way in range(2):
            for kind in range(2):
                at = wrap(self.me1(kind) - u * (1 - 2 * way))
                if u < 4 - way and not self.direct:
                    self.near_copy(kind, way, u, at).start()
        self.open_chunk(u - 1)

    def far_step(self, s, j):
        self.arrived(self.far.at[s - 1, j], 8 if s < 4 else 4)
        for way in range(2):
            for kind in range(2):
                at2 = wrap(self.me2(kind) - s * (1 - 2 * way))
                if s < 3 or (s == 3 and j % 2 == way):
                    self.far_copy(kind, way, s, j, at2).start()

    def far_steps(self, s):
        for j in range(4):
            self.far_step(s, j)

    def finish(self):
        for kind in range(2):
            for i, part in enumerate((self.arrays[kind].at[0, 0:7], self.arrays[kind].at[0:7])):
                pltpu.make_async_remote_copy(
                    src_ref=part, dst_ref=part, send_sem=self.send.at[kind, i],
                    recv_sem=self.near.at[0],
                    device_id=self.device(True, 1), device_id_type=MESH).wait_send()


def kernel(
    lam_ref, hgain_ref, ngain_ref, res_hbm, q_hbm, key_hbm, val_hbm, ow_hbm, up_hbm, down_hbm,
    out_ref,
    kv_a, kv_b, up_a, up_b, dn_a, dn_b, res_ref, ow_ref, q_all, st_all, ho_all, an_all, sq_all,
    pre_out, pre_in, rs_out, rs_all, keep, o_scr, mix_a, mix_b, got_a, got_b,
    kv_send, kv_near, kv_far, u_send, u_near, u_far, d_send, d_near, d_far,
    x_send, x_recv, x_chip, pre_send, pre_recv, in_sem,
):
    sp, tp = lax.axis_index("sp"), lax.axis_index("tp")
    z, y = lax.div(sp, RING), lax.rem(sp, RING)
    x, c = lax.div(tp, 2), lax.rem(tp, 2)
    partner = x * 2 + 1 - c
    kv = Gather(kv_a, kv_b, y, z, tp, (kv_send, kv_near, kv_far), True)
    w1 = Gather(up_a, up_b, y, z, tp, (u_send, u_near, u_far), False)
    w2 = Gather(dn_a, dn_b, y, z, tp, (d_send, d_near, d_far), False)

    barrier = pltpu.get_barrier_semaphore()

    @pl.loop(1, RING)
    def _(p):
        pl.semaphore_signal(barrier, inc=1, device_id=(sp, wrap(tp + p)), device_id_type=MESH)
        for along_y in (True, False):
            pl.semaphore_signal(barrier, inc=1, device_id=kv.device(along_y, p), device_id_type=MESH)

    loads = [
        pltpu.make_async_copy(src, dst, in_sem.at[i])
        for i, (src, dst) in enumerate((
            (key_hbm.at[:, 0:256], kv_a.at[z, y, :, 0:256]),
            (val_hbm.at[:, 0:256], kv_a.at[z, y, :, 256:512]),
            (key_hbm.at[:, 256:512], kv_b.at[y, z, :, 0:256]),
            (val_hbm.at[:, 256:512], kv_b.at[y, z, :, 256:512]),
            (q_hbm, q_all.at[tp]),
            (up_hbm.at[:, 0:512], up_a.at[z, y]),
            (up_hbm.at[:, 512:1024], up_b.at[y, z]),
            (down_hbm.at[0:16], dn_a.at[z, y]),
            (down_hbm.at[16:32], dn_b.at[y, z]),
            (res_hbm, res_ref),
            (ow_hbm, ow_ref),
        ))
    ]
    for load in loads:
        load.start()
    pl.semaphore_wait(barrier, TP - 1 + 2 * (RING - 1))

    def chip(step):
        return lax.rem(x + step + 4, 4)

    def tp_of(step):
        return chip(step) * 2 + c

    def x_copy(k, src, dst, slot, peer, sem=None):
        return pltpu.make_async_remote_copy(
            src_ref=src, dst_ref=dst.at[slot], send_sem=x_send.at[k],
            recv_sem=x_recv.at[k] if sem is None else sem, device_id=(sp, peer), device_id_type=MESH)

    def x_all(k, part):
        pltpu.make_async_remote_copy(
            src_ref=part, dst_ref=part, send_sem=x_send.at[k], recv_sem=x_recv.at[k],
            device_id=(sp, partner), device_id_type=MESH).wait_recv()

    def share(k, array):
        for step in (2, 1, 3):
            x_copy(k, array.at[tp], array, tp, tp_of(step), x_chip.at[k % 4, x]).start()
        x_copy(k, array.at[tp], array, tp, partner).start()

    def relay(k, array):
        for step in (1, 3, 2):
            slot = tp_of(step)
            x_copy(k, array.at[slot], array, slot, partner, x_chip.at[k % 4, chip(step)]).wait_recv()
            x_copy(k, array.at[slot], array, slot, partner).start()

    def collect(k, array):
        x_all(k, array.at[0:4])

    def x_sent(k, part):
        pltpu.make_async_remote_copy(
            src_ref=part, dst_ref=part, send_sem=x_send.at[k], recv_sem=x_recv.at[k],
            device_id=(sp, partner), device_id_type=MESH).wait_send()

    events = [(w1, 1, j) for j in range(4)]
    for j in range(4):
        events += [(w2, 0, j + 1), (w1, 2, j)]
    for j in range(4):
        events += [(w1, 3, j), (w2, 1, j)]
    for j in range(4):
        events += [(w1, 4, j), (w2, 2, j)]

    def pump(count):
        for _ in range(count):
            gather, s, j = events.pop(0)
            if s == 0:
                gather.near_step(j)
            else:
                gather.far_step(s, j)

    for load in loads[0:5]:
        load.wait()
    kv.begin()
    share(0, q_all)
    for load in loads[5:11]:
        load.wait()
    w1.begin()
    for u in range(1, 5):
        kv.near_step(u)
    for s in range(1, 4):
        kv.far_steps(s)
        if s == 1:
            relay(0, q_all)
        w1.near_step(s)
    w2.begin()
    kv.far_steps(4)
    w1.near_step(4)
    collect(0, q_all)

    lane = lax.broadcasted_iota(jnp.int32, (ROWS, 128), 1)
    stats = jnp.zeros((ROWS, 128), F32)
    for gc in range(4):
        g, m_c = gc // 2, gc % 2
        whole = kv_a if g == 0 else kv_b
        q = q_all[4 * g : 4 * g + 4, :, m_c * 128 : m_c * 128 + 128].reshape(4 * ROWS, 128)
        k = whole[:, :, :, m_c * 128 : m_c * 128 + 128].reshape(1024, 128)
        v = whole[:, :, :, 256:512].reshape(1024, 256)
        s = lax.dot_general(q, k, NT, preferred_element_type=F32)
        m = jnp.max(s, axis=1, keepdims=True)
        p = jnp.exp2((s - m) * LOG_SCALE)
        t = jnp.sum(p, axis=1, keepdims=True)
        o = jnp.dot(p.astype(BF16), v, preferred_element_type=F32)
        m = m * LOG_SCALE
        for i in range(4):
            at = (4 * g + i) * 2 + m_c
            o_scr[at] = o[i * ROWS : (i + 1) * ROWS]
            stats = jnp.where(lane == at, m[i * ROWS : (i + 1) * ROWS], stats)
            stats = jnp.where(lane == at + 16, t[i * ROWS : (i + 1) * ROWS], stats)
        pump(1)

    st_all[tp] = jnp.transpose(stats)[0:32]
    pump(1)
    for step in (2, 1, 3):
        for core in range(2):
            x_copy(1, st_all.at[tp], st_all, tp, chip(step) * 2 + core).start()
    x_copy(1, st_all.at[tp], st_all, tp, partner).start()
    pump(3)
    x_all(1, st_all.at[0:7])

    every = st_all[...]
    maxima, totals = every[:, 0:16], every[:, 16:32]
    highest = jnp.max(maxima, axis=0)
    total = jnp.sum(jnp.exp2(maxima - highest[None]) * totals, axis=0)
    mine = st_all[tp]
    coef = jnp.exp2(mine[0:16] - highest) / total
    row = lax.broadcasted_iota(jnp.int32, (16, 128), 0)
    factor = jnp.ones((16, 128), F32)
    for h in range(HEADS):
        factor = jnp.where(row == 2 * h + 1, -lam_ref[h], factor)
    coef = jnp.concatenate([coef * factor, jnp.zeros((112, 128), F32)], axis=0)
    coef = jnp.transpose(coef)

    def differ(i, h):
        even = lax.rem(h, 2) == 0
        first = jnp.where(even, coef[:, 4 * i : 4 * i + 1], coef[:, 4 * i + 2 : 4 * i + 3])
        second = jnp.where(even, coef[:, 4 * i + 1 : 4 * i + 2], coef[:, 4 * i + 3 : 4 * i + 4])
        return o_scr[2 * h] * first + o_scr[2 * h + 1] * second

    for i in range(4):
        pre_out[i] = differ(i, 2 * i + 1 - c).astype(BF16)
    across = pltpu.make_async_remote_copy(
        src_ref=pre_out, dst_ref=pre_in, send_sem=pre_send, recv_sem=pre_recv,
        device_id=(sp, partner), device_id_type=MESH)
    across.start()
    pump(1)
    for i in range(4):
        keep[i] = differ(i, 2 * i + c)
    pump(1)
    across.wait_recv()
    for step in (2, 1, 3):
        i = chip(step)
        rs_out[i] = (keep[i] + pre_in[i].astype(F32)).astype(BF16)
    for step in (2, 1, 3):
        i = chip(step)
        x_copy(2, rs_out.at[i], rs_all, x, tp_of(step)).start()
    difference = keep[x] + pre_in[x].astype(F32)
    pump(5)
    x_all(2, rs_all.at[0:3])
    for step in (1, 3, 2):
        difference += rs_all[chip(step)].astype(F32)

    square = jnp.mean(difference * difference, axis=-1, keepdims=True)
    ho_all[tp] = (difference * lax.rsqrt(square + EPSILON) * hgain_ref[...]).astype(BF16)
    pump(1)
    share(3, ho_all)
    pump(3)
    relay(3, ho_all)
    pump(1)
    collect(3, ho_all)
    heads = jnp.concatenate([ho_all[h] for h in range(HEADS)], axis=1)
    projected = jnp.dot(heads, ow_ref[...], preferred_element_type=F32)
    after_mix = res_ref[...].astype(F32) + projected
    keep[0] = after_mix
    an_all[tp] = (after_mix * ngain_ref[...]).astype(BF16)
    squares = jnp.sum(after_mix * after_mix, axis=1, keepdims=True)
    sq_all[tp] = jnp.transpose(jnp.broadcast_to(squares, (ROWS, 128)))[0:8]
    pump(1)
    share(9, an_all)
    share(10, sq_all)
    pump(4)
    relay(9, an_all)
    relay(10, sq_all)
    pump(1)
    collect(9, an_all)
    collect(10, sq_all)
    squares = jnp.sum(sq_all[...], axis=0)
    squares = jnp.transpose(jnp.broadcast_to(squares[0:1], (128, 128)))[:, 0:1]
    scale = lax.rsqrt(squares / D + EPSILON)
    pump(len(events))

    normed = jnp.concatenate([an_all[t] for t in range(TP)], axis=1)
    parts = []
    for half in range(2):
        if half == 0:
            weights = up_a[...].reshape(2048, 512)
        else:
            weights = jnp.concatenate([up_b[:, t].reshape(256, 512) for t in range(TP)], axis=0)
        hidden = jnp.dot(normed, weights, preferred_element_type=F32) * scale
        parts.append(jnp.square(jax.nn.relu(hidden)).astype(BF16))
    activated = jnp.concatenate(parts, axis=1)

    def mix(weights):
        return lax.dot_general(
            activated, weights.reshape(128, 1024), NT, preferred_element_type=F32).astype(BF16)

    def give(k, out, got, t):
        @pl.when(t != tp)
        def _():
            x_copy(k, out.at[t], got, tp, t).start()

        @pl.when(t == tp)
        def _():
            got[tp] = out[tp]

    def give_a(places):
        for t in places:
            mix_a[t] = mix(dn_a[t])
        for t in places:
            give(6, mix_a, got_a, t)

    def mix_block(d):
        block = dn_b[wrap(y + offsets[d])].reshape(128, 1024)
        sums = lax.dot_general(block, activated, NT, preferred_element_type=F32)
        mix_b[:, d] = sums.astype(BF16).reshape(TP, 16, 128)

    def b_copy(k, t, part):
        return pltpu.make_async_remote_copy(
            src_ref=mix_b.at[t, part], dst_ref=got_b.at[tp, part], send_sem=x_send.at[k],
            recv_sem=x_recv.at[k], device_id=(sp, t), device_id_type=MESH)

    def give_b(k, part):
        for step in (2, 1, 3):
            for core in range(2):
                b_copy(k, chip(step) * 2 + core, part).start()
        b_copy(k, partner, part).start()

    offsets = (0, 1, -1, 2, -2, 3, -3, 4)
    early, late = pl.ds(0, 7), pl.ds(7, 1)
    give_a([z])
    give_a([wrap(z + 1), wrap(z - 1)])
    for d in range(3):
        mix_block(d)
    give_a([wrap(z + 2), wrap(z - 2)])
    for d in range(3, 5):
        mix_block(d)
    for j in range(4):
        w2.far_step(3, j)
    give_a([wrap(z + 3), wrap(z - 3)])
    for d in range(5, 7):
        mix_block(d)
    give_b(7, early)
    for j in range(4):
        w2.far_step(4, j)
    mix_block(7)
    give_a([wrap(z + 4)])
    give_b(8, late)
    got_b[tp] = mix_b[tp]

    x_all(6, got_a.at[0:7])

    source = lax.broadcasted_iota(jnp.int32, (128, 256), 0)
    target = lax.broadcasted_iota(jnp.int32, (128, 256), 1)
    at = lax.div(source, 16) * 32 + lax.rem(source, 16)
    spread = jnp.where(at == target, 1.0, 0.0).astype(BF16)
    rows = jnp.concatenate([got_a[t] for t in range(TP)], axis=1)
    total = jnp.dot(rows, jnp.concatenate([spread] * TP, axis=0), preferred_element_type=F32)
    keep[0] = keep[0] + total

    target = lax.broadcasted_iota(jnp.int32, (256, 128), 0)
    source = lax.broadcasted_iota(jnp.int32, (256, 128), 1)
    d = lax.div(source, 16)
    at = y + lax.div(d + 1, 2) * (2 * lax.rem(d, 2) - 1)
    at = lax.rem(at + RING, RING) * 32 + 16 + lax.rem(source, 16)
    spread = jnp.where(at == target, 1.0, 0.0).astype(BF16)
    x_all(7, got_b.at[0:7, 0:7])
    x_all(8, got_b.at[0, 0:7])
    total = jnp.dot(
        jnp.concatenate([spread] * TP, axis=1), got_b[...].reshape(TP * 128, 128), preferred_element_type=F32)
    out_ref[...] = (keep[0] + jnp.transpose(total)).astype(BF16)

    kv.finish()
    w1.finish()
    w2.finish()
    for k, array in ((0, q_all), (1, st_all), (3, ho_all), (9, an_all), (10, sq_all), (6, mix_a)):
        x_sent(k, array.at[0:7])
    x_sent(2, rs_out.at[0:3])
    x_sent(7, mix_b.at[0:7, 0:7])
    x_sent(8, mix_b.at[0, 0:7])
    across.wait_send()


def on_device(residual, queries, key_proj, value_proj, diff_lambda, head_gain, out_weight, norm_gain, up_weight, down_weight):
    vmem = pl.BlockSpec(memory_space=pltpu.VMEM)
    smem = pl.BlockSpec(memory_space=pltpu.SMEM)
    hbm = pl.BlockSpec(memory_space=pltpu.HBM)
    block = (TP, ROWS, 256)
    half = (TP, ROWS, 128)
    dma = pltpu.SemaphoreType.DMA
    return pl.pallas_call(
        kernel,
        out_shape=jax.ShapeDtypeStruct((ROWS, 256), BF16),
        in_specs=[smem, vmem, vmem] + [hbm] * 7,
        out_specs=vmem,
        scratch_shapes=[
            pltpu.VMEM((RING, RING, 16, 512), BF16),
            pltpu.VMEM((RING, RING, 16, 512), BF16),
            pltpu.VMEM((RING, RING, 32, 512), BF16),
            pltpu.VMEM((RING, RING, 32, 512), BF16),
            pltpu.VMEM((RING, RING, 16, 1024), BF16),
            pltpu.VMEM((RING, RING, 16, 1024), BF16),
            pltpu.VMEM((ROWS, 256), BF16),
            pltpu.VMEM((2048, 256), BF16),
            pltpu.VMEM(block, BF16),
            pltpu.VMEM((TP, 32, 128), F32),
            pltpu.VMEM(block, BF16),
            pltpu.VMEM(block, BF16),
            pltpu.VMEM((TP, 8, 128), F32),
            pltpu.VMEM((4, ROWS, 256), BF16),
            pltpu.VMEM((4, ROWS, 256), BF16),
            pltpu.VMEM((4, ROWS, 256), BF16),
            pltpu.VMEM((4, ROWS, 256), BF16),
            pltpu.VMEM((4, ROWS, 256), F32),
            pltpu.VMEM((16, ROWS, 256), F32),
            pltpu.VMEM(half, BF16),
            pltpu.VMEM((TP, 8, 16, 128), BF16),
            pltpu.VMEM(half, BF16),
            pltpu.VMEM((TP, 8, 16, 128), BF16),
            dma((2, 2)), dma((4,)), dma((4, 4)),
            dma((2, 2)), dma((4,)), dma((4, 4)),
            dma((2, 2)), dma((4,)), dma((4, 4)),
            dma((11,)), dma((11,)), dma((4, 4)), dma, dma, dma((11,)),
        ],
        compiler_params=pltpu.CompilerParams(
            collective_id=0, has_side_effects=True, vmem_limit_bytes=67043328),
    )(diff_lambda, head_gain.reshape(1, 256), norm_gain.reshape(1, 256), residual, queries, key_proj, value_proj,
      out_weight, up_weight, down_weight.T)


def solution(mesh):
    return jax.shard_map(
        on_device,
        mesh=mesh,
        in_specs=(
            P("sp", "tp"),
            P("sp", "tp"),
            P(("sp", "tp"), None),
            P(("sp", "tp"), None),
            P(),
            P(),
            P(None, "tp"),
            P("tp"),
            P("sp", "tp"),
            P("tp", "sp"),
        ),
        out_specs=P("sp", "tp"),
        check_vma=False,
    )
```

```python
import jax
import jax.numpy as jnp
from jax import lax
from jax.experimental import pallas as pl
from jax.experimental.pallas import tpu as pltpu
from jax.sharding import PartitionSpec as P

D = 2048
HEADS = 8
HEAD_DIM = 128
RING = 8
TP = 8
ROWS = 128
EPSILON = 1e-06
MESH = pl.DeviceIdType.MESH
F32 = jnp.float32
BF16 = jnp.bfloat16
LOG_SCALE = HEAD_DIM ** (-0.5) * 1.4426950408889634
NT = (((1,), (1,)), ((), ()))


def wrap(i):
    return lax.rem(i + RING, RING)


class Gather:
    def __init__(self, first, second, y, z, tp, sems, direct, long=0):
        self.arrays = (first, second)
        self.y, self.z, self.tp = y, z, tp
        self.send, self.near, self.far = sems
        self.direct, self.long = direct, long

    def me1(self, kind):
        return self.y if kind == 0 else self.z

    def me2(self, kind):
        return self.z if kind == 0 else self.y

    def device(self, along_y, step):
        if along_y:
            return (self.z * RING + wrap(self.y + step), self.tp)
        return (wrap(self.z + step) * RING + self.y, self.tp)

    def near_copy(self, kind, way, s, at):
        c = self.arrays[kind].at[self.me2(kind), at]
        step = (1 - 2 * way) * (s + 1 if self.direct else 1)
        return pltpu.make_async_remote_copy(
            src_ref=c, dst_ref=c, send_sem=self.send.at[kind, 0], recv_sem=self.near.at[s],
            device_id=self.device(kind == 0, step), device_id_type=MESH)

    def far_copy(self, kind, way, s, j, at2):
        c = self.arrays[kind].at[at2, pl.ds(2 * self.place(kind, j), 2)]
        return pltpu.make_async_remote_copy(
            src_ref=c, dst_ref=c, send_sem=self.send.at[kind, 1], recv_sem=self.far.at[s, j],
            device_id=self.device(kind == 1, 1 - 2 * way), device_id_type=MESH)

    def place(self, kind, j):
        me = self.me1(kind)
        pair, side = lax.div(me, 2), 1 - 2 * lax.rem(me, 2)
        offset = (0, -side, side, 2)[j]
        return lax.rem(pair + offset + 4, 4)

    def open_chunk(self, j):
        for kind in range(2):
            for way in range(2):
                self.far_copy(kind, way, 0, j, self.me2(kind)).start()

    def begin(self):
        for s in range(4 if self.direct else 1):
            for kind in range(2):
                for way in range(2) if s < 3 else (self.long,):
                    self.near_copy(kind, way, s, self.me1(kind)).start()

    def arrived(self, sem, shards):
        part = self.arrays[0].at[0, 0:shards]
        pltpu.make_async_remote_copy(
            src_ref=part, dst_ref=part, send_sem=self.send.at[0, 0], recv_sem=sem,
            device_id=self.device(True, 1), device_id_type=MESH).wait_recv()

    def near_step(self, u):
        self.arrived(self.near.at[u - 1], 4 if u < 4 else 2)
        for way in range(2):
            for kind in range(2):
                at = wrap(self.me1(kind) - u * (1 - 2 * way))
                if u < (4 if way == self.long else 3) and not self.direct:
                    self.near_copy(kind, way, u, at).start()
        self.open_chunk(u - 1)

    def far_step(self, s, j):
        self.arrived(self.far.at[s - 1, j], 8 if s < 4 else 4)
        for way in range(2):
            for kind in range(2):
                at2 = wrap(self.me2(kind) - s * (1 - 2 * way))
                if s < 3 or (s == 3 and j % 2 == way):
                    self.far_copy(kind, way, s, j, at2).start()

    def far_steps(self, s):
        for j in range(4):
            self.far_step(s, j)

    def finish(self):
        for kind in range(2):
            for i, part in enumerate((self.arrays[kind].at[0, 0:7], self.arrays[kind].at[0:7])):
                pltpu.make_async_remote_copy(
                    src_ref=part, dst_ref=part, send_sem=self.send.at[kind, i],
                    recv_sem=self.near.at[0],
                    device_id=self.device(True, 1), device_id_type=MESH).wait_send()


def kernel(
    lam_ref, hgain_ref, ngain_ref, res_hbm, q_hbm, key_hbm, val_hbm, ow_hbm, up_hbm, down_hbm,
    out_ref,
    kv_a, kv_b, up_a, up_b, dn_a, dn_b, res_ref, ow_ref, q_all, st_all, ho_all, an_all, sq_all,
    pre_out, pre_in, rs_out, rs_all, keep, o_scr, mix_a, mix_b, got_a, got_b,
    kv_send, kv_near, kv_far, u_send, u_near, u_far, d_send, d_near, d_far,
    x_send, x_recv, x_chip, pre_send, pre_recv, in_sem,
):
    sp, tp = lax.axis_index("sp"), lax.axis_index("tp")
    z, y = lax.div(sp, RING), lax.rem(sp, RING)
    x, c = lax.div(tp, 2), lax.rem(tp, 2)
    partner = x * 2 + 1 - c
    kv = Gather(kv_a, kv_b, y, z, tp, (kv_send, kv_near, kv_far), True)
    w1 = Gather(up_a, up_b, y, z, tp, (u_send, u_near, u_far), False)
    w2 = Gather(dn_a, dn_b, y, z, tp, (d_send, d_near, d_far), False, 1)

    barrier = pltpu.get_barrier_semaphore()

    @pl.loop(1, RING)
    def _(p):
        pl.semaphore_signal(barrier, inc=1, device_id=(sp, wrap(tp + p)), device_id_type=MESH)
        for along_y in (True, False):
            pl.semaphore_signal(barrier, inc=1, device_id=kv.device(along_y, p), device_id_type=MESH)

    loads = [
        pltpu.make_async_copy(src, dst, in_sem.at[i])
        for i, (src, dst) in enumerate((
            (key_hbm.at[:, 0:256], kv_a.at[z, y, :, 0:256]),
            (val_hbm.at[:, 0:256], kv_a.at[z, y, :, 256:512]),
            (key_hbm.at[:, 256:512], kv_b.at[y, z, :, 0:256]),
            (val_hbm.at[:, 256:512], kv_b.at[y, z, :, 256:512]),
            (q_hbm, q_all.at[tp]),
            (up_hbm.at[:, 0:512], up_a.at[z, y]),
            (up_hbm.at[:, 512:1024], up_b.at[y, z]),
            (down_hbm.at[0:16], dn_a.at[z, y]),
            (down_hbm.at[16:32], dn_b.at[y, z]),
            (res_hbm, res_ref),
            (ow_hbm, ow_ref),
        ))
    ]
    for load in loads:
        load.start()
    pl.semaphore_wait(barrier, TP - 1 + 2 * (RING - 1))

    def chip(step):
        return lax.rem(x + step + 4, 4)

    def tp_of(step):
        return chip(step) * 2 + c

    def x_copy(k, src, dst, slot, peer, sem=None):
        return pltpu.make_async_remote_copy(
            src_ref=src, dst_ref=dst.at[slot], send_sem=x_send.at[k],
            recv_sem=x_recv.at[k] if sem is None else sem, device_id=(sp, peer), device_id_type=MESH)

    def x_all(k, part):
        pltpu.make_async_remote_copy(
            src_ref=part, dst_ref=part, send_sem=x_send.at[k], recv_sem=x_recv.at[k],
            device_id=(sp, partner), device_id_type=MESH).wait_recv()

    def share(k, array):
        for step in (2, 1, 3):
            x_copy(k, array.at[tp], array, tp, tp_of(step), x_chip.at[k % 4, x]).start()
        x_copy(k, array.at[tp], array, tp, partner).start()

    def relay(k, array):
        for step in (1, 3, 2):
            slot = tp_of(step)
            x_copy(k, array.at[slot], array, slot, partner, x_chip.at[k % 4, chip(step)]).wait_recv()
            x_copy(k, array.at[slot], array, slot, partner).start()

    def collect(k, array):
        x_all(k, array.at[0:4])

    def x_sent(k, part):
        pltpu.make_async_remote_copy(
            src_ref=part, dst_ref=part, send_sem=x_send.at[k], recv_sem=x_recv.at[k],
            device_id=(sp, partner), device_id_type=MESH).wait_send()

    events = [(w1, 1, j) for j in range(4)]
    for j in range(4):
        events += [(w2, 0, j + 1), (w1, 2, j)]
    for j in range(4):
        events += [(w1, 3, j), (w2, 1, j)]
    for j in range(4):
        events += [(w1, 4, j), (w2, 2, j)]

    def pump(count):
        for _ in range(count):
            gather, s, j = events.pop(0)
            if s == 0:
                gather.near_step(j)
            else:
                gather.far_step(s, j)

    for load in loads[0:5]:
        load.wait()
    kv.begin()
    share(0, q_all)
    for load in loads[5:11]:
        load.wait()
    w1.begin()
    for u in range(1, 5):
        kv.near_step(u)
    for s in range(1, 4):
        kv.far_steps(s)
        if s == 1:
            relay(0, q_all)
        w1.near_step(s)
    w2.begin()
    kv.far_steps(4)
    w1.near_step(4)
    collect(0, q_all)

    lane = lax.broadcasted_iota(jnp.int32, (ROWS, 128), 1)
    stats = jnp.zeros((ROWS, 128), F32)
    for gc in range(4):
        g, m_c = gc // 2, gc % 2
        whole = kv_a if g == 0 else kv_b
        q = q_all[4 * g : 4 * g + 4, :, m_c * 128 : m_c * 128 + 128].reshape(4 * ROWS, 128)
        k = whole[:, :, :, m_c * 128 : m_c * 128 + 128].reshape(1024, 128)
        v = whole[:, :, :, 256:512].reshape(1024, 256)
        s = lax.dot_general(q, k, NT, preferred_element_type=F32)
        m = jnp.max(s, axis=1, keepdims=True)
        p = jnp.exp2((s - m) * LOG_SCALE)
        t = jnp.sum(p, axis=1, keepdims=True)
        o = jnp.dot(p.astype(BF16), v, preferred_element_type=F32)
        m = m * LOG_SCALE
        for i in range(4):
            at = (4 * g + i) * 2 + m_c
            o_scr[at] = o[i * ROWS : (i + 1) * ROWS]
            stats = jnp.where(lane == at, m[i * ROWS : (i + 1) * ROWS], stats)
            stats = jnp.where(lane == at + 16, t[i * ROWS : (i + 1) * ROWS], stats)
        pump(1)

    st_all[tp] = jnp.transpose(stats)[0:32]
    pump(1)
    for step in (2, 1, 3):
        for core in range(2):
            x_copy(1, st_all.at[tp], st_all, tp, chip(step) * 2 + core).start()
    x_copy(1, st_all.at[tp], st_all, tp, partner).start()
    pump(3)
    x_all(1, st_all.at[0:7])

    every = st_all[...]
    maxima, totals = every[:, 0:16], every[:, 16:32]
    highest = jnp.max(maxima, axis=0)
    total = jnp.sum(jnp.exp2(maxima - highest[None]) * totals, axis=0)
    mine = st_all[tp]
    coef = jnp.exp2(mine[0:16] - highest) / total
    row = lax.broadcasted_iota(jnp.int32, (16, 128), 0)
    factor = jnp.ones((16, 128), F32)
    for h in range(HEADS):
        factor = jnp.where(row == 2 * h + 1, -lam_ref[h], factor)
    coef = jnp.concatenate([coef * factor, jnp.zeros((112, 128), F32)], axis=0)
    coef = jnp.transpose(coef)

    def differ(i, h):
        even = lax.rem(h, 2) == 0
        first = jnp.where(even, coef[:, 4 * i : 4 * i + 1], coef[:, 4 * i + 2 : 4 * i + 3])
        second = jnp.where(even, coef[:, 4 * i + 1 : 4 * i + 2], coef[:, 4 * i + 3 : 4 * i + 4])
        return o_scr[2 * h] * first + o_scr[2 * h + 1] * second

    for i in range(4):
        pre_out[i] = differ(i, 2 * i + 1 - c).astype(BF16)
    across = pltpu.make_async_remote_copy(
        src_ref=pre_out, dst_ref=pre_in, send_sem=pre_send, recv_sem=pre_recv,
        device_id=(sp, partner), device_id_type=MESH)
    across.start()
    pump(1)
    for i in range(4):
        keep[i] = differ(i, 2 * i + c)
    pump(1)
    across.wait_recv()
    for step in (2, 1, 3):
        i = chip(step)
        rs_out[i] = (keep[i] + pre_in[i].astype(F32)).astype(BF16)
    for step in (2, 1, 3):
        i = chip(step)
        x_copy(2, rs_out.at[i], rs_all, x, tp_of(step)).start()
    difference = keep[x] + pre_in[x].astype(F32)
    pump(5)
    x_all(2, rs_all.at[0:3])
    for step in (1, 3, 2):
        difference += rs_all[chip(step)].astype(F32)

    square = jnp.mean(difference * difference, axis=-1, keepdims=True)
    ho_all[tp] = (difference * lax.rsqrt(square + EPSILON) * hgain_ref[...]).astype(BF16)
    pump(1)
    share(3, ho_all)
    pump(3)
    relay(3, ho_all)
    pump(1)
    collect(3, ho_all)
    heads = jnp.concatenate([ho_all[h] for h in range(HEADS)], axis=1)
    projected = jnp.dot(heads, ow_ref[...], preferred_element_type=F32)
    after_mix = res_ref[...].astype(F32) + projected
    keep[0] = after_mix
    an_all[tp] = (after_mix * ngain_ref[...]).astype(BF16)
    squares = jnp.sum(after_mix * after_mix, axis=1, keepdims=True)
    sq_all[tp] = jnp.transpose(jnp.broadcast_to(squares, (ROWS, 128)))[0:8]
    pump(1)
    share(9, an_all)
    share(10, sq_all)
    pump(4)
    relay(9, an_all)
    relay(10, sq_all)
    pump(1)
    collect(9, an_all)
    collect(10, sq_all)
    squares = jnp.sum(sq_all[...], axis=0)
    squares = jnp.transpose(jnp.broadcast_to(squares[0:1], (128, 128)))[:, 0:1]
    scale = lax.rsqrt(squares / D + EPSILON)
    pump(len(events))

    normed = jnp.concatenate([an_all[t] for t in range(TP)], axis=1)
    parts = []
    for half in range(2):
        if half == 0:
            weights = up_a[...].reshape(2048, 512)
        else:
            weights = jnp.concatenate([up_b[:, t].reshape(256, 512) for t in range(TP)], axis=0)
        hidden = jnp.dot(normed, weights, preferred_element_type=F32) * scale
        parts.append(jnp.square(jax.nn.relu(hidden)).astype(BF16))
    activated = jnp.concatenate(parts, axis=1)

    def mix(weights):
        return lax.dot_general(
            activated, weights.reshape(128, 1024), NT, preferred_element_type=F32).astype(BF16)

    def give(k, out, got, t):
        @pl.when(t != tp)
        def _():
            x_copy(k, out.at[t], got, tp, t).start()

        @pl.when(t == tp)
        def _():
            got[tp] = out[tp]

    def give_a(places):
        for t in places:
            mix_a[t] = mix(dn_a[t])
        for t in places:
            give(6, mix_a, got_a, t)

    def mix_block(d):
        block = dn_b[wrap(y + offsets[d])].reshape(128, 1024)
        sums = lax.dot_general(block, activated, NT, preferred_element_type=F32)
        mix_b[:, d] = sums.astype(BF16).reshape(TP, 16, 128)

    def b_copy(k, t, part):
        return pltpu.make_async_remote_copy(
            src_ref=mix_b.at[t, part], dst_ref=got_b.at[tp, part], send_sem=x_send.at[k],
            recv_sem=x_recv.at[k], device_id=(sp, t), device_id_type=MESH)

    def give_b(k, part):
        for step in (2, 1, 3):
            for core in range(2):
                b_copy(k, chip(step) * 2 + core, part).start()
        b_copy(k, partner, part).start()

    offsets = (0, 1, -1, 2, -2, 3, -3, 4)
    early, late = pl.ds(0, 7), pl.ds(7, 1)
    give_a([z])
    give_a([wrap(z + 1), wrap(z - 1)])
    for d in range(3):
        mix_block(d)
    give_a([wrap(z + 2), wrap(z - 2)])
    for d in range(3, 5):
        mix_block(d)
    for j in range(4):
        w2.far_step(3, j)
    give_a([wrap(z + 3), wrap(z - 3)])
    for d in range(5, 7):
        mix_block(d)
    give_b(7, early)
    for j in range(4):
        w2.far_step(4, j)
    mix_block(7)
    give_a([wrap(z + 4)])
    give_b(8, late)
    got_b[tp] = mix_b[tp]

    x_all(6, got_a.at[0:7])

    source = lax.broadcasted_iota(jnp.int32, (128, 256), 0)
    target = lax.broadcasted_iota(jnp.int32, (128, 256), 1)
    at = lax.div(source, 16) * 32 + lax.rem(source, 16)
    spread = jnp.where(at == target, 1.0, 0.0).astype(BF16)
    rows = jnp.concatenate([got_a[t] for t in range(TP)], axis=1)
    total = jnp.dot(rows, jnp.concatenate([spread] * TP, axis=0), preferred_element_type=F32)
    keep[0] = keep[0] + total

    target = lax.broadcasted_iota(jnp.int32, (256, 128), 0)
    source = lax.broadcasted_iota(jnp.int32, (256, 128), 1)
    d = lax.div(source, 16)
    at = y + lax.div(d + 1, 2) * (2 * lax.rem(d, 2) - 1)
    at = lax.rem(at + RING, RING) * 32 + 16 + lax.rem(source, 16)
    spread = jnp.where(at == target, 1.0, 0.0).astype(BF16)
    x_all(7, got_b.at[0:7, 0:7])
    x_all(8, got_b.at[0, 0:7])
    total = jnp.dot(
        jnp.concatenate([spread] * TP, axis=1), got_b[...].reshape(TP * 128, 128), preferred_element_type=F32)
    out_ref[...] = (keep[0] + jnp.transpose(total)).astype(BF16)

    kv.finish()
    w1.finish()
    w2.finish()
    for k, array in ((0, q_all), (1, st_all), (3, ho_all), (9, an_all), (10, sq_all), (6, mix_a)):
        x_sent(k, array.at[0:7])
    x_sent(2, rs_out.at[0:3])
    x_sent(7, mix_b.at[0:7, 0:7])
    x_sent(8, mix_b.at[0, 0:7])
    across.wait_send()


def on_device(residual, queries, key_proj, value_proj, diff_lambda, head_gain, out_weight, norm_gain, up_weight, down_weight):
    vmem = pl.BlockSpec(memory_space=pltpu.VMEM)
    smem = pl.BlockSpec(memory_space=pltpu.SMEM)
    hbm = pl.BlockSpec(memory_space=pltpu.HBM)
    block = (TP, ROWS, 256)
    half = (TP, ROWS, 128)
    dma = pltpu.SemaphoreType.DMA
    return pl.pallas_call(
        kernel,
        out_shape=jax.ShapeDtypeStruct((ROWS, 256), BF16),
        in_specs=[smem, vmem, vmem] + [hbm] * 7,
        out_specs=vmem,
        scratch_shapes=[
            pltpu.VMEM((RING, RING, 16, 512), BF16),
            pltpu.VMEM((RING, RING, 16, 512), BF16),
            pltpu.VMEM((RING, RING, 32, 512), BF16),
            pltpu.VMEM((RING, RING, 32, 512), BF16),
            pltpu.VMEM((RING, RING, 16, 1024), BF16),
            pltpu.VMEM((RING, RING, 16, 1024), BF16),
            pltpu.VMEM((ROWS, 256), BF16),
            pltpu.VMEM((2048, 256), BF16),
            pltpu.VMEM(block, BF16),
            pltpu.VMEM((TP, 32, 128), F32),
            pltpu.VMEM(block, BF16),
            pltpu.VMEM(block, BF16),
            pltpu.VMEM((TP, 8, 128), F32),
            pltpu.VMEM((4, ROWS, 256), BF16),
            pltpu.VMEM((4, ROWS, 256), BF16),
            pltpu.VMEM((4, ROWS, 256), BF16),
            pltpu.VMEM((4, ROWS, 256), BF16),
            pltpu.VMEM((4, ROWS, 256), F32),
            pltpu.VMEM((16, ROWS, 256), F32),
            pltpu.VMEM(half, BF16),
            pltpu.VMEM((TP, 8, 16, 128), BF16),
            pltpu.VMEM(half, BF16),
            pltpu.VMEM((TP, 8, 16, 128), BF16),
            dma((2, 2)), dma((4,)), dma((4, 4)),
            dma((2, 2)), dma((4,)), dma((4, 4)),
            dma((2, 2)), dma((4,)), dma((4, 4)),
            dma((11,)), dma((11,)), dma((4, 4)), dma, dma, dma((11,)),
        ],
        compiler_params=pltpu.CompilerParams(
            collective_id=0, has_side_effects=True, vmem_limit_bytes=67043328),
    )(diff_lambda, head_gain.reshape(1, 256), norm_gain.reshape(1, 256), residual, queries, key_proj, value_proj,
      out_weight, up_weight, down_weight.T)


def solution(mesh):
    return jax.shard_map(
        on_device,
        mesh=mesh,
        in_specs=(
            P("sp", "tp"),
            P("sp", "tp"),
            P(("sp", "tp"), None),
            P(("sp", "tp"), None),
            P(),
            P(),
            P(None, "tp"),
            P("tp"),
            P("sp", "tp"),
            P("tp", "sp"),
        ),
        out_specs=P("sp", "tp"),
        check_vma=False,
    )
```
